512 devices in a mesh: ep: 32 (over z, x), tp: 16 (over y, core).
Axes of the slice: x: 4, y: 8, z: 8, core: 2. Of those that a mesh axis runs over, the one named last changes fastest.
Arguments:
- tokens: bfloat16 [8192, 4096], P('ep', 'tp'), may hold values from -72 to 72
- pre_gain: float32 [4096], P('tp'), may hold values from 0.1 to 1.9
- expert_ids: int32 [8192, 3], P('ep'), may hold values from 0 to 63, all different within a row; in each aligned block of 256 rows (0 to 255, 256 to 511, ...) at most 16 rows name the same one
- route_weight: float32 [8192, 3], P('ep'), may hold values from 0.2 to 2
- expert_gate: bfloat16 [64, 1024, 4096], P('ep', 'tp'), may hold values from -0.09375 to 0.09375
- expert_up: bfloat16 [64, 1024, 4096], P('ep', 'tp'), may hold values from -0.09375 to 0.09375
- expert_down: bfloat16 [64, 1024, 4096], P('ep', None, 'tp'), may hold values from -0.9375 to 0.9375
- shared_gate: bfloat16 [1024, 4096], P('tp'), may hold values from -0.09375 to 0.09375
- shared_up: bfloat16 [1024, 4096], P('tp'), may hold values from -0.09375 to 0.09375
- shared_down: bfloat16 [1024, 4096], P(None, 'tp'), may hold values from -0.9375 to 0.9375
- out_gain: float32 [4096], P('tp'), may hold values from 0.1 to 1.9
Outputs:
- mixed: bfloat16 [8192, 4096], P('ep', 'tp')
The draws below stay inside these ranges and needn't reach their ends.
Inputs may be any that keep to these rules, and one draw needn't show every extreme that they name: `expert_ids`: A row names 3 different experts. Among the rows of one index of ep no expert is named more than 16 times, and in every draw some expert is named exactly 16 times there.
All inputs are finite; a program needn't handle non-finite values.
Results may differ from the reference program's by a relative error of at most 0.0068.
Values may be sent and summed in bfloat16 or wider, within the bound.
No kernel may reach another device: no remote copies, remote signals or barrier semaphores. Data moves between devices by JAX's collectives and lax.ppermute only.
A program may use at most 64 MiB of HBM per device.

```python
import math
import jax
import jax.numpy as jnp
import numpy as np
from jax import lax

D = 4096
F = 1024
FS = 1024
TOK = 256
TOP = 3
EXPERTS = 64
CAP = 16
TOKENS = 8192
N_EP = 32


def column_ramp(key, top_ratio):
    ramp = jnp.exp(jnp.linspace(0.0, math.log(top_ratio), D)).astype(jnp.float32)
    rough = jax.random.uniform(key, (D,), jnp.float32, 0.5, 1.5)
    return ramp * rough


def base_values(key, shape):
    values = jnp.clip(jax.random.normal(key, shape, jnp.float32), -4.0, 4.0)
    return values


def draw_tokens(key, part):
    key_col, key_row, key_val = jax.random.split(jax.random.fold_in(key, 101), 3)
    column = column_ramp(key_col, 6.0)
    row_scale = jnp.exp(jax.random.uniform(key_row, (TOKENS, 1), jnp.float32, 0.0, math.log(8.0)))
    values = base_values(key_val, (TOKENS, D))
    return (values * column[None, :] * row_scale * 0.25).astype(jnp.bfloat16)


def draw_expert_down(key, part):
    key_col, key_val = jax.random.split(jax.random.fold_in(key, 202), 2)
    column = column_ramp(key_col, 5.0)
    values = base_values(key_val, (EXPERTS, F, D))
    return (values * column[None, None, :] * F ** (-0.5)).astype(jnp.bfloat16)


def draw_shared_down(key, part):
    key_col, key_val = jax.random.split(jax.random.fold_in(key, 303), 2)
    column = column_ramp(key_col, 5.0)
    values = base_values(key_val, (FS, D))
    return (values * column[None, :] * FS ** (-0.5)).astype(jnp.bfloat16)


def block_scale(stream_key, dims, shards, least, top_value):
    level, own = 1.0, jax.random.fold_in(stream_key, 6)
    for axis_at, parts in shards:
        draws = jnp.exp(jax.random.uniform(jax.random.fold_in(own, axis_at), (parts,), jnp.float32, least / len(shards), top_value / len(shards)))
        level = level * jnp.repeat(draws, dims[axis_at] // parts).reshape([-1 if axis == axis_at else 1 for axis in range(len(dims))])
    return level


def deal_out(own_key, own, number, rows, amount, top, reach, skew):
    ranking = jax.random.permutation(own_key, amount)
    heavy_load, common = portions_of(amount, rows * top, reach, skew, True), portions_of(amount, rows * top, reach, skew, False)
    places = jnp.arange(amount)

    def named(sizes, offset_by):
        used = int((sizes > 0).sum())
        fixed = max(1, used // 4)
        moved = fixed + (places - fixed + offset_by * (used - fixed)) % max(1, amount - fixed)
        return jnp.zeros((amount,), jnp.int32).at[ranking[jnp.where(places < fixed, places, moved)]].set(jnp.asarray(sizes, jnp.int32))

    sizes = jnp.where(number % 4 == 0, named(heavy_load, number // 4), named(common, number - number // 4 - 1))
    mixed = jax.random.permutation(jax.random.fold_in(own, 3), amount)
    donor, sink = mixed[0:amount // 2 * 2:2], mixed[1:amount // 2 * 2:2]
    room = jnp.minimum(sizes[donor] - 1, reach - sizes[sink]) // 2
    room = jnp.where((donor == ranking[0]) | (sink == ranking[0]) | (sizes[sink] == 0), 0, jnp.maximum(room, 0))
    moved = jax.random.randint(jax.random.fold_in(own, 4), (amount // 2,), 0, 1 << 20) % (room + 1)
    sizes = sizes.at[donor].add(-moved).at[sink].add(moved)
    members = jnp.searchsorted(jnp.cumsum(sizes), jnp.arange(rows * top), side="right").astype(jnp.int32)
    table = members.reshape(top, rows).T
    table = table[jax.random.permutation(jax.random.fold_in(own, 1), rows)]
    offset_by = jax.random.randint(jax.random.fold_in(own, 2), (rows, 1), 0, top)
    return jnp.take_along_axis(table, (jnp.arange(top)[None, :] + offset_by) % top, axis=1)


def portions_of(count, total, bound, skew, full):
    portions = [(1 << 20) // math.isqrt(standing ** skew) + 1 for standing in range(1, count + 1)]
    largest = bound if full else min(bound, max(-(-total // count), total * portions[0] // sum(portions)))
    least = 1 if total - largest >= count - 1 else 0
    counts, spare = [largest] + [least] * (count - 1), total - largest - least * (count - 1)
    while spare > 0:
        candidates = [i for i in range(1, count) if counts[i] < largest] or [i for i in range(1, count) if counts[i] < bound]
        whole, remaining = sum([portions[i] for i in candidates]), spare
        for i in candidates:
            more = min(bound - counts[i], max(1, remaining * portions[i] // whole), spare)
            counts[i] = counts[i] + more
            spare = spare - more
    return np.array(counts)


def normal_values(key, extent, spread, bound, cuts=(), held_as=jnp.bfloat16):
    level = block_scale(key, extent, cuts, -0.22, 0.18) if cuts else 1.0
    result = jax.random.normal(key, extent, jnp.float32) * spread * level
    return jnp.minimum(jnp.maximum(result, -bound), bound).astype(held_as)


def setup_inputs(seed: int = 0) -> dict:
    key_of = jax.random.split(jax.random.key(seed), 12)
    tokens = draw_tokens(jax.random.fold_in(key_of[11], 71), 0)
    pre_gain = jnp.clip(1.0 + 0.18 * jax.random.normal(key_of[1], (D,), jnp.float32), 0.1, 1.9)
    expert_ids_keys = jax.random.split(jax.random.fold_in(key_of[2], 1), TOKENS // TOK)
    expert_ids_turns = jax.random.permutation(jax.random.fold_in(key_of[2], 3), TOKENS // TOK)
    expert_ids = jax.vmap(lambda own, number: deal_out(jax.random.fold_in(key_of[2], 2), own, number, TOK, EXPERTS, TOP, CAP, 2))(expert_ids_keys, expert_ids_turns).reshape((TOKENS, TOP))
    route_weight = jnp.clip(jnp.exp(math.log(2.0) - 2.3025851 * jax.random.uniform(key_of[3], (TOKENS, TOP), jnp.float32) ** block_scale(key_of[3], (TOKENS, TOP), ((0, 32),), -0.2, 0.2)), 0.2, 2.0)
    expert_gate = normal_values(key_of[4], (EXPERTS, F, D), D ** -0.5, 0.09375, ((0, 32), (1, 16)))
    expert_up = normal_values(key_of[5], (EXPERTS, F, D), D ** -0.5, 0.09375, ((0, 32), (1, 16)))
    expert_down = draw_expert_down(jax.random.fold_in(key_of[11], 71), 0)
    shared_gate = normal_values(key_of[7], (FS, D), D ** -0.5, 0.09375, ((0, 16),))
    shared_up = normal_values(key_of[8], (FS, D), D ** -0.5, 0.09375, ((0, 16),))
    shared_down = draw_shared_down(jax.random.fold_in(key_of[11], 71), 0)
    out_gain = jnp.clip(1.0 + 0.18 * jax.random.normal(key_of[10], (D,), jnp.float32), 0.1, 1.9)
    return {"tokens": tokens, "pre_gain": pre_gain, "expert_ids": expert_ids, "route_weight": route_weight, "expert_gate": expert_gate, "expert_up": expert_up, "expert_down": expert_down, "shared_gate": shared_gate, "shared_up": shared_up, "shared_down": shared_down, "out_gain": out_gain}


EPSILON = 1e-06

def norm_rows(values, gain):
    scale = lax.rsqrt(lax.optimization_barrier(jnp.mean(values * values, axis=-1, keepdims=True)) + EPSILON)
    return values * scale * gain

def reference(tokens, pre_gain, expert_ids, route_weight, expert_gate, expert_up, expert_down, shared_gate, shared_up, shared_down, out_gain):
    normed = norm_rows(tokens.astype(jnp.float32), pre_gain).astype(jnp.bfloat16)
    flat_ids = expert_ids.reshape(N_EP, TOK * TOP).astype(jnp.int32)
    one_hot = (flat_ids[:, :, None] == jnp.arange(EXPERTS, dtype=jnp.int32)[None, None, :]).astype(jnp.int32)
    before = jnp.cumsum(one_hot, axis=1) - one_hot
    slot_index = lax.optimization_barrier(jnp.sum(before * one_hot, axis=2)).astype(jnp.int32)
    dest_index = (flat_ids * CAP + slot_index).astype(jnp.int32)
    block_index = jnp.arange(N_EP, dtype=jnp.int32)[:, None]
    order = jnp.broadcast_to(jnp.arange(TOK * TOP, dtype=jnp.int32)[None, :], (N_EP, TOK * TOP))
    source = jnp.full((N_EP, EXPERTS * CAP), -1, jnp.int32).at[block_index, dest_index].set(order)
    is_live = source >= 0
    row_index = (jnp.where(is_live, source // TOP, 0) + block_index * TOK).astype(jnp.int32)
    row_index = row_index.reshape(N_EP, EXPERTS, CAP).transpose(1, 0, 2).reshape(EXPERTS, N_EP * CAP)
    is_live = is_live.reshape(N_EP, EXPERTS, CAP).transpose(1, 0, 2).reshape(EXPERTS, N_EP * CAP)

    def one_expert(operands):
        expert_rows, expert_live, weight_gate, weight_up, weight_down = operands
        buffer = normed[expert_rows] * expert_live[:, None].astype(jnp.bfloat16)
        gate_sum = jnp.dot(buffer, weight_gate.T, preferred_element_type=jnp.float32)
        up_sum = jnp.dot(buffer, weight_up.T, preferred_element_type=jnp.float32)
        hidden_act = (jax.nn.silu(gate_sum) * up_sum).astype(jnp.bfloat16)
        return jnp.dot(hidden_act, weight_down, preferred_element_type=jnp.float32).astype(jnp.bfloat16)
    results = lax.map(one_expert, (row_index, is_live, expert_gate, expert_up, expert_down))
    results = results.reshape(EXPERTS * N_EP * CAP, D)
    lookup = (flat_ids * (N_EP * CAP) + block_index * CAP + slot_index).reshape(TOKENS * TOP).astype(jnp.int32)
    picked = results[lookup].reshape(TOKENS, TOP, D).astype(jnp.float32)
    routed = lax.optimization_barrier(jnp.sum(picked * route_weight[:, :, None], axis=1))
    shared_gate_sum = jnp.dot(normed, shared_gate.T, preferred_element_type=jnp.float32)
    shared_up_sum = jnp.dot(normed, shared_up.T, preferred_element_type=jnp.float32)
    shared_act = (jax.nn.silu(shared_gate_sum) * shared_up_sum).astype(jnp.bfloat16)
    shared_out = jnp.dot(shared_act, shared_down, preferred_element_type=jnp.float32)
    summed = routed + shared_out
    return norm_rows(summed, out_gain).astype(jnp.bfloat16)
```

```python
import jax
import jax.numpy as jnp
from jax import lax
from jax.sharding import PartitionSpec as P

EPSILON = 1e-06
BF = jnp.bfloat16
F32 = jnp.float32


def on_device(
    tokens,
    pre_gain,
    expert_ids,
    route_weight,
    expert_gate,
    expert_up,
    expert_down,
    shared_gate,
    shared_up,
    shared_down,
    out_gain,
):
    tok, top = expert_ids.shape
    n_ep = lax.axis_size("ep")
    n_tp = lax.axis_size("tp")
    n_y = n_tp // 2
    experts = expert_gate.shape[0] * n_ep
    cap = 4 * tok * top // (3 * experts)
    feat = tokens.shape[1]
    feat_all = feat * n_tp
    hid = expert_gate.shape[1]
    half = tok // 2
    slots = n_ep * cap
    rows = slots + half
    tp = lax.axis_index("tp")
    core = lax.rem(tp, 2)
    y = lax.div(tp, 2)
    first = core == 0

    swap = [(i, i ^ 1) for i in range(n_tp)]
    y_groups = [[c + 2 * k for k in range(n_y)] for c in range(2)]

    def y_shift(d):
        return [(i, ((i // 2 + d) % n_y) * 2 + i % 2) for i in range(n_tp)]

    def own_first(mine, other, axis):
        return jnp.where(
            first,
            jnp.concatenate([mine, other], axis=axis),
            jnp.concatenate([other, mine], axis=axis),
        )

    def sum_over_tp(v):
        sent = jnp.broadcast_to(v[None, :], (n_tp, v.shape[0]))
        return jnp.sum(lax.all_to_all(sent, "tp", 0, 0, tiled=True), axis=0)

    tok_float = tokens.astype(F32)
    square_sum = sum_over_tp(jnp.sum(tok_float * tok_float, axis=1))
    normed = (tok_float * lax.rsqrt(square_sum[:, None] / feat_all + EPSILON) * pre_gain).astype(BF)
    normed = own_first(normed, lax.ppermute(normed, "tp", swap), 1)

    other_core = 1 - core
    sent_in = jnp.concatenate(
        [
            lax.dynamic_index_in_dim(expert_gate, other_core, 0, keepdims=False),
            lax.dynamic_index_in_dim(expert_up, other_core, 0, keepdims=False),
            shared_gate,
            shared_up,
        ],
        axis=0,
    )
    sent_out = jnp.concatenate(
        [lax.dynamic_index_in_dim(expert_down, other_core, 0, keepdims=False), shared_down], axis=0
    )
    got_in = lax.ppermute(sent_in, "tp", swap)
    got_out = lax.ppermute(sent_out, "tp", swap)
    gate_w = own_first(lax.dynamic_index_in_dim(expert_gate, core, 0, keepdims=False), got_in[:hid], 0)
    up_w = own_first(lax.dynamic_index_in_dim(expert_up, core, 0, keepdims=False), got_in[hid : 2 * hid], 0)
    in_w = jnp.concatenate([gate_w, up_w], axis=0)
    sgate_w = own_first(shared_gate, got_in[2 * hid : 3 * hid], 0)
    sup_w = own_first(shared_up, got_in[3 * hid :], 0)
    sin_w = jnp.concatenate([sgate_w, sup_w], axis=0)
    n_hid = expert_down.shape[1]
    down_w = own_first(lax.dynamic_index_in_dim(expert_down, core, 0, keepdims=False), got_out[:n_hid], 1)
    sdown_w = own_first(shared_down, got_out[n_hid:], 1)

    ids = expert_ids.T
    named = 2 * jnp.arange(n_ep, dtype=jnp.int32)[:, None] + core
    hit = [(ids[k][None, :] == named) for k in range(top)]
    member = (hit[0] | hit[1] | hit[2])
    earlier = (
        jnp.arange(tok, dtype=jnp.int32)[:, None] < jnp.arange(tok, dtype=jnp.int32)[None, :]
    ).astype(BF)
    rank = jnp.dot(member.astype(BF), earlier, preferred_element_type=F32)
    rank = jnp.where(member, rank, -1.0)
    slot_no = jnp.arange(cap, dtype=jnp.int32).astype(F32)
    pick = rank[:, None, :] == slot_no[None, :, None]
    weight = sum(jnp.where(hit[k], route_weight.T[k][None, :], 0.0) for k in range(top))
    one_hot = pick.astype(BF).reshape(slots, tok)
    outgoing = jnp.dot(one_hot, normed, preferred_element_type=F32).astype(BF)
    arrived = lax.all_to_all(outgoing.reshape(n_ep, cap, 2 * feat), "ep", 0, 0, tiled=True)
    mine = lax.dynamic_slice_in_dim(normed, core * half, half, 0)
    chunk = jnp.concatenate([arrived.reshape(slots, 2 * feat), mine], axis=0)

    n_sub = rows // 2
    cut = [chunk[:n_sub], chunk[n_sub:]]
    width = 2 * feat

    def w_at(w, pos):
        return lax.dynamic_slice(w, (0, pos * width), (w.shape[0], width))

    def mult(x, w):
        return lax.dot_general(x, w, (((1,), (1,)), ((), ())), preferred_element_type=F32)

    def products(part, which, pos):
        if which == 0:
            return [mult(part, w_at(in_w, pos))]
        split = slots - n_sub
        return [mult(part[:split], w_at(in_w, pos)), mult(part[split:], w_at(sin_w, pos))]

    def add(a, b):
        return b if a is None else [p + q for p, q in zip(a, b)]

    total = [None, None]
    for k in range(2):
        total[k] = products(cut[k], k, y)
    fwd, bwd = list(cut), list(cut)
    for step in range(1, n_y // 2 + 1):
        for k in range(2):
            last = step == n_y // 2
            if not last or k == 0:
                fwd[k] = lax.ppermute(fwd[k], "tp", y_shift(1))
                total[k] = add(total[k], products(fwd[k], k, lax.rem(y + n_y - step, n_y)))
            if not last or k == 1:
                bwd[k] = lax.ppermute(bwd[k], "tp", y_shift(-1))
                total[k] = add(total[k], products(bwd[k], k, lax.rem(y + step, n_y)))

    def act(s):
        gate, up = s[:, : 2 * hid], s[:, 2 * hid :]
        return (jax.nn.silu(gate) * up).astype(BF)

    hidden = jnp.concatenate([act(total[0][0]), act(total[1][0]), act(total[1][1])], axis=0)
    spread = jnp.broadcast_to(hidden[None], (n_y,) + hidden.shape)
    hidden_all = lax.all_to_all(spread, "tp", 0, 0, axis_index_groups=y_groups, tiled=True)
    down_w = down_w.reshape(n_y, 2 * hid, width)
    sdown_w = sdown_w.reshape(n_y, 2 * hid, width)
    contract = (((0, 2), (0, 1)), ((), ()))
    expert_out = lax.dot_general(
        hidden_all[:, :slots], down_w, contract, preferred_element_type=F32
    ).astype(BF)
    shared_out = lax.dot_general(hidden_all[:, slots:], sdown_w, contract, preferred_element_type=F32)
    returned = lax.all_to_all(expert_out.reshape(n_ep, cap, width), "ep", 0, 0, tiled=True)
    returned = returned.reshape(slots, width)

    mix = jnp.where(pick, weight[:, None, :], 0.0).reshape(slots, tok)
    high = lax.reduce_precision(mix, 8, 7)
    middle = lax.reduce_precision(mix - high, 8, 7)
    low = mix - high - middle
    part = sum(
        lax.dot_general(m.astype(BF), returned, (((0,), (0,)), ((), ())), preferred_element_type=F32)
        for m in (high, middle, low)
    )
    zero = jnp.zeros_like(shared_out)
    part = part + jnp.where(
        first,
        jnp.concatenate([shared_out, zero], axis=0),
        jnp.concatenate([zero, shared_out], axis=0),
    )
    away = jnp.where(first, part[:, feat:], part[:, :feat])
    home = jnp.where(first, part[:, :feat], part[:, feat:])
    summed = home + lax.ppermute(away, "tp", swap)
    out_square = sum_over_tp(jnp.sum(summed * summed, axis=1))
    return (summed * lax.rsqrt(out_square[:, None] / feat_all + EPSILON) * out_gain).astype(BF)


def solution(mesh):
    return jax.shard_map(
        on_device,
        mesh=mesh,
        in_specs=(
            P("ep", "tp"),
            P("tp"),
            P("ep", None),
            P("ep", None),
            P("ep", "tp", None),
            P("ep", "tp", None),
            P("ep", None, "tp"),
            P("tp", None),
            P("tp", None),
            P(None, "tp"),
            P("tp"),
        ),
        out_specs=P("ep", "tp"),
        check_vma=False,
    )
```

```python
import functools

import jax
import jax.numpy as jnp
from jax import lax
from jax.experimental import pallas as pl
from jax.experimental.pallas import tpu as pltpu
from jax.sharding import PartitionSpec as P


EPSILON = 1e-06
BF = jnp.bfloat16
F32 = jnp.float32


VMEM = pl.BlockSpec(memory_space=pltpu.VMEM)
SMEM = pl.BlockSpec(memory_space=pltpu.SMEM)


def after(x, *first):
    return lax.optimization_barrier((x,) + first)[0]


def times(x, w):
    return lax.dot_general(x, w, (((1,), (1,)), ((), ())), preferred_element_type=F32)


def product(pieces, places, spans, n_y, width, y, w_refs, half, total):
    for piece, (k, offset) in zip(pieces, places):
        if k != half:
            continue
        at = pl.multiple_of(lax.rem(y + offset + n_y, n_y) * width, width)
        for i, (low, high, which) in enumerate(spans[half]):
            term = times(piece[low:high, :], w_refs[which][:, pl.ds(at, width)])
            total[i] = term if total[i] is None else total[i] + term
    return total


def early_kernel(places, spans, n_y, width, y_ref, w_ref, sw_ref, *refs):
    out_ref = refs[-1]
    n_sub = out_ref.shape[0] // 2
    for half in range(2):
        total = [None] * len(spans[half])
        total = product(refs[:-1], places, spans, n_y, width, y_ref[0], (w_ref, sw_ref), half, total)
        for (low, high, _), value in zip(spans[half], total):
            out_ref[half * n_sub + low : half * n_sub + high, :] = value


def late_kernel(places, spans, n_y, width, y_ref, w_ref, sw_ref, total_ref, scale_ref, *refs):
    out_ref = refs[-1]
    n_sub = out_ref.shape[0] // 2
    for half in range(2):
        at = [slice(half * n_sub + low, half * n_sub + high) for low, high, _ in spans[half]]
        total = [total_ref[rows, :] for rows in at]
        total = product(refs[:-1], places, spans, n_y, width, y_ref[0], (w_ref, sw_ref), half, total)
        for rows, value in zip(at, total):
            out_ref[rows, :] = activated(value * scale_ref[rows, :])


def activated(total):
    n = total.shape[1] // 2
    gate, up = total[:, :n], total[:, n:]
    return (gate / (1.0 + jnp.exp(-gate)) * up).astype(BF)


def call(kernel, out, flops, args, smem=0):
    size = sum(a.size * a.dtype.itemsize for a in args)
    return pl.pallas_call(
        kernel,
        out_shape=out,
        in_specs=[SMEM] * smem + [VMEM] * (len(args) - smem),
        out_specs=VMEM,
        cost_estimate=pl.CostEstimate(flops=flops, bytes_accessed=size, transcendentals=0),
    )(*args)


def body(
    tokens,
    pre_gain,
    expert_ids,
    route_weight,
    expert_gate,
    expert_up,
    expert_down,
    shared_gate,
    shared_up,
    shared_down,
    out_gain,
):
    tok, top = expert_ids.shape
    n_ep = lax.axis_size("ep")
    n_tp = lax.axis_size("tp")
    n_y = n_tp // 2
    experts = expert_gate.shape[0] * n_ep
    cap = 4 * tok * top // (3 * experts)
    feat = tokens.shape[1]
    feat_all = feat * n_tp
    width = 2 * feat
    hid = expert_gate.shape[1]
    n_hid = expert_down.shape[1]
    half = tok // 2
    slots = n_ep * cap
    tp = lax.axis_index("tp")
    core = lax.rem(tp, 2)
    y = lax.div(tp, 2)
    first = core == 0
    other_core = 1 - core

    swap = [(i, i ^ 1) for i in range(n_tp)]
    y_groups = [[c + 2 * k for k in range(n_y)] for c in range(2)]

    def y_shift(d):
        return [(i, ((i // 2 + d) % n_y) * 2 + i % 2) for i in range(n_tp)]

    def own_first(mine, other, axis):
        return jnp.where(
            first,
            jnp.concatenate([mine, other], axis=axis),
            jnp.concatenate([other, mine], axis=axis),
        )

    def to_all_y(v):
        sent = jnp.broadcast_to(v[None], (n_y,) + v.shape)
        return lax.all_to_all(sent, "tp", 0, 0, axis_index_groups=y_groups, tiled=True)

    whole = own_first(tokens, lax.ppermute(tokens, "tp", swap), 1)
    ids = expert_ids.T
    named = 2 * jnp.arange(n_ep, dtype=jnp.int32)[:, None] + core
    hit = [(ids[k][None, :] == named) for k in range(top)]
    member = hit[0] | hit[1] | hit[2]
    earlier = (
        jnp.arange(tok, dtype=jnp.int32)[:, None] < jnp.arange(tok, dtype=jnp.int32)[None, :]
    ).astype(BF)
    rank = jnp.dot(member.astype(BF), earlier, preferred_element_type=F32)
    rank = jnp.where(member, rank, -1.0)
    slot_no = jnp.arange(cap, dtype=jnp.int32).astype(F32)
    pick = rank[:, None, :] == slot_no[None, :, None]
    one_hot = pick.astype(BF).reshape(slots, tok)
    outgoing = jnp.dot(one_hot, whole, preferred_element_type=F32).astype(BF)
    arrived = lax.all_to_all(outgoing.reshape(n_ep, cap, width), "ep", 0, 0, tiled=True)
    arrived = arrived.reshape(slots, width)

    gain = own_first(pre_gain, lax.ppermute(after(pre_gain, outgoing), "tp", swap), 0)
    own_rows = lax.dynamic_slice_in_dim(whole, core * half, half, 0)

    e_gate, e_up, s_gate, s_up, _ = lax.optimization_barrier((expert_gate, expert_up, shared_gate, shared_up, outgoing))
    sent_in = jnp.concatenate(
        [
            lax.dynamic_index_in_dim(e_gate, other_core, 0, keepdims=False),
            lax.dynamic_index_in_dim(e_up, other_core, 0, keepdims=False),
            s_gate,
            s_up,
        ],
        axis=0,
    )
    got_in = lax.ppermute(sent_in, "tp", swap)
    in_w = jnp.concatenate(
        [
            own_first(lax.dynamic_index_in_dim(e_gate, core, 0, keepdims=False), got_in[:hid], 0),
            own_first(
                lax.dynamic_index_in_dim(e_up, core, 0, keepdims=False), got_in[hid : 2 * hid], 0
            ),
        ],
        axis=0,
    )
    sin_w = jnp.concatenate(
        [own_first(s_gate, got_in[2 * hid : 3 * hid], 0), own_first(s_up, got_in[3 * hid :], 0)],
        axis=0,
    )
    e_down, s_down, _ = lax.optimization_barrier((expert_down, shared_down, outgoing))
    sent_out = jnp.concatenate(
        [lax.dynamic_index_in_dim(e_down, other_core, 0, keepdims=False), s_down], axis=0
    )
    got_out = lax.ppermute(sent_out, "tp", swap)
    down_w = own_first(
        lax.dynamic_index_in_dim(e_down, core, 0, keepdims=False), got_out[:n_hid], 1
    ).reshape(n_y, 2 * hid, width)
    sdown_w = own_first(s_down, got_out[n_hid:], 1).reshape(n_y, 2 * hid, width)

    rows = slots + half
    n_sub = rows // 2
    raw = jnp.concatenate([arrived, own_rows], axis=0).astype(F32)
    chunk = (raw * gain).astype(BF)
    square = jnp.sum(raw * raw, axis=1)
    spans = (((0, n_sub, 0),), ((0, slots - n_sub, 0), (slots - n_sub, n_sub, 1)))
    fwd = [chunk[:n_sub], chunk[n_sub:]]
    bwd = list(fwd)
    early, early_at = list(fwd), [(0, 0), (1, 0)]
    late, late_at = [], []
    for step in range(1, n_y // 2 + 1):
        last = step == n_y // 2
        pieces, at = (late, late_at) if last else (early, early_at)
        for k in range(2):
            if not last or k == 0:
                fwd[k] = lax.ppermute(fwd[k], "tp", y_shift(1))
                pieces.append(fwd[k])
                at.append((k, -step))
            if not last or k == 1:
                bwd[k] = lax.ppermute(bwd[k], "tp", y_shift(-1))
                pieces.append(bwd[k])
                at.append((k, step))
        if step == 1:
            square_sum = jnp.sum(to_all_y(after(square, fwd[0])), axis=0)
            scale = lax.rsqrt(square_sum / feat_all + EPSILON)[:, None]

    where = y[None].astype(jnp.int32)
    flops = 2 * rows * feat_all * 4 * hid
    total = call(
        functools.partial(early_kernel, early_at, spans, n_y, width),
        jax.ShapeDtypeStruct((rows, 4 * hid), F32),
        flops,
        (where, in_w, sin_w, *early),
        smem=1,
    )
    hidden = call(
        functools.partial(late_kernel, late_at, spans, n_y, width),
        jax.ShapeDtypeStruct((rows, 2 * hid), BF),
        flops // n_y,
        (where, in_w, sin_w, total, scale, *late),
        smem=1,
    )

    hidden_all = to_all_y(hidden)
    contract = (((0, 2), (0, 1)), ((), ()))
    expert_out = lax.dot_general(hidden_all[:, :slots], down_w, contract, preferred_element_type=F32).astype(BF)
    returned = lax.all_to_all(expert_out.reshape(n_ep, cap, width), "ep", 0, 0, tiled=True)
    returned = returned.reshape(slots, width)

    shared_out = lax.dot_general(hidden_all[:, slots:], sdown_w, contract, preferred_element_type=F32)
    weight = sum(jnp.where(hit[k], route_weight.T[k][None, :], 0.0) for k in range(top))
    mix = jnp.where(pick, weight[:, None, :], 0.0).reshape(slots, tok)
    high = lax.reduce_precision(mix, 8, 7)
    middle = lax.reduce_precision(mix - high, 8, 7)
    low = mix - high - middle
    part = sum(
        lax.dot_general(m.astype(BF), returned, (((0,), (0,)), ((), ())), preferred_element_type=F32)
        for m in (high, middle, low)
    )
    zero = jnp.zeros_like(shared_out)
    part = part + jnp.where(
        first,
        jnp.concatenate([shared_out, zero], axis=0),
        jnp.concatenate([zero, shared_out], axis=0),
    )
    away = jnp.where(first, part[:, feat:], part[:, :feat])
    home = jnp.where(first, part[:, :feat], part[:, feat:])
    summed = home + lax.ppermute(away, "tp", swap)
    own_square = jnp.sum(summed * summed, axis=1)
    sent = jnp.broadcast_to(own_square[None, :], (n_tp, tok))
    out_square = jnp.sum(lax.all_to_all(sent, "tp", 0, 0, tiled=True), axis=0)
    return (summed * lax.rsqrt(out_square[:, None] / feat_all + EPSILON) * out_gain).astype(BF)


def solution(mesh):
    return jax.shard_map(
        body,
        mesh=mesh,
        in_specs=(
            P("ep", "tp"),
            P("tp"),
            P("ep", None),
            P("ep", None),
            P("ep", "tp", None),
            P("ep", "tp", None),
            P("ep", None, "tp"),
            P("tp", None),
            P("tp", None),
            P(None, "tp"),
            P("tp"),
        ),
        out_specs=P("ep", "tp"),
        check_vma=False,
    )
```

```python
import functools

import jax
import jax.numpy as jnp
from jax import lax
from jax.experimental import pallas as pl
from jax.experimental.pallas import tpu as pltpu
from jax.sharding import PartitionSpec as P


EPSILON = 1e-06
BF = jnp.bfloat16
F32 = jnp.float32


VMEM = pl.BlockSpec(memory_space=pltpu.VMEM)
SMEM = pl.BlockSpec(memory_space=pltpu.SMEM)
HBM = pl.BlockSpec(memory_space=pltpu.HBM)


def after(x, *first):
    return lax.optimization_barrier((x,) + first)[0]


def times(x, w):
    return lax.dot_general(x, w, (((1,), (1,)), ((), ())), preferred_element_type=F32)


def early_kernel(places, spans, n_y, width, at_ref, gate, up, s_gate, s_up, got, *refs):
    n = len(places)
    pieces = refs[:n]
    total_ref, w_last, sw_last = refs[n : n + 3]
    w, sw, held, w_sem, sem = refs[n + 3 :]
    core, y = at_ref[0], at_ref[1]
    hid = s_gate.shape[0]
    n_sub = total_ref.shape[0] // 2
    own = pl.multiple_of(core * hid, hid)
    other = pl.multiple_of((1 - core) * hid, hid)
    moves = []
    for i, (mine, into, base) in enumerate(
        ((gate.at[core], w, 0), (up.at[core], w, 2 * hid), (s_gate, sw, 0), (s_up, sw, 2 * hid))
    ):
        moves.append(pltpu.make_async_copy(mine, into.at[pl.ds(base + own, hid)], w_sem.at[2 * i]))
        theirs = got.at[pl.ds(i * hid, hid)]
        moves.append(pltpu.make_async_copy(theirs, into.at[pl.ds(base + other, hid)], w_sem.at[2 * i + 1]))
    loads = [pltpu.make_async_copy(p, held.at[i], sem.at[i]) for i, p in enumerate(pieces)]
    for copy in moves + loads:
        copy.start()
    for copy in moves:
        copy.wait()
    for half in range(2):
        total = [None] * len(spans[half])
        for i, (k, offset) in enumerate(places):
            if k != half:
                continue
            loads[i].wait()
            at = pl.multiple_of(lax.rem(y + offset + n_y, n_y) * width, width)
            for j, (low, high, which) in enumerate(spans[half]):
                term = times(held[i, low:high, :], (w, sw)[which][:, pl.ds(at, width)])
                total[j] = term if total[j] is None else total[j] + term
        for (low, high, _), value in zip(spans[half], total):
            total_ref[half * n_sub + low : half * n_sub + high, :] = value
    at = pl.multiple_of(lax.rem(y + n_y // 2, n_y) * width, width)
    w_last[...] = w[:, pl.ds(at, width)]
    sw_last[...] = sw[:, pl.ds(at, width)]


def late_kernel(spans, w_ref, sw_ref, total_ref, scale_ref, *refs):
    out_ref = refs[-1]
    n_sub = total_ref.shape[0] // 2
    for half in range(2):
        for low, high, which in spans[half]:
            rows = slice(half * n_sub + low, half * n_sub + high)
            total = total_ref[rows, :] + times(refs[half][low:high, :], (w_ref, sw_ref)[which][...])
            hidden = activated(total * scale_ref[rows, :])
            for j in range(out_ref.shape[0]):
                out_ref[j, rows, :] = hidden


def pack_kernel(at_ref, *refs):
    n = len(refs) - 3
    arrays, out_ref, held, sem = refs[:n], refs[n], refs[n + 1], refs[n + 2]
    rows = out_ref.shape[0] // n
    ins = []
    for i, a in enumerate(arrays):
        part = a.at[1 - at_ref[0]] if len(a.shape) == 3 else a
        ins.append(pltpu.make_async_copy(part, held.at[pl.ds(i * rows, rows)], sem.at[i]))
    outs = [
        pltpu.make_async_copy(
            held.at[pl.ds(i * rows, rows)], out_ref.at[pl.ds(i * rows, rows)], sem.at[n + i]
        )
        for i in range(n)
    ]
    for copy in ins:
        copy.start()
    for i in range(n):
        ins[i].wait()
        outs[i].start()
    for copy in outs:
        copy.wait()


def pack(at, arrays):
    rows, cols = arrays[0].shape[-2:]
    shape = (rows * len(arrays), cols)
    return pl.pallas_call(
        pack_kernel,
        out_shape=jax.ShapeDtypeStruct(shape, BF),
        in_specs=[SMEM] + [HBM] * len(arrays),
        out_specs=HBM,
        scratch_shapes=[pltpu.VMEM(shape, BF), pltpu.SemaphoreType.DMA((2 * len(arrays),))],
        cost_estimate=pl.CostEstimate(flops=4 * 10**8, bytes_accessed=2**22, transcendentals=0),
        compiler_params=pltpu.CompilerParams(vmem_limit_bytes=4 * 2**20),
    )(at, *arrays)


def activated(total):
    n = total.shape[1] // 2
    gate, up = total[:, :n], total[:, n:]
    return (gate / (1.0 + jnp.exp(-gate)) * up).astype(BF)


def body(
    tokens,
    pre_gain,
    expert_ids,
    route_weight,
    expert_gate,
    expert_up,
    expert_down,
    shared_gate,
    shared_up,
    shared_down,
    out_gain,
):
    tok, top = expert_ids.shape
    n_ep = lax.axis_size("ep")
    n_tp = lax.axis_size("tp")
    n_y = n_tp // 2
    experts = expert_gate.shape[0] * n_ep
    cap = 4 * tok * top // (3 * experts)
    feat = tokens.shape[1]
    feat_all = feat * n_tp
    width = 2 * feat
    hid = expert_gate.shape[1]
    n_hid = expert_down.shape[1]
    half = tok // 2
    slots = n_ep * cap
    tp = lax.axis_index("tp")
    core = lax.rem(tp, 2)
    y = lax.div(tp, 2)
    first = core == 0

    place = jnp.stack([core, y]).astype(jnp.int32)
    swap = [(i, i ^ 1) for i in range(n_tp)]
    y_groups = [[c + 2 * k for k in range(n_y)] for c in range(2)]

    def y_shift(d):
        return [(i, ((i // 2 + d) % n_y) * 2 + i % 2) for i in range(n_tp)]

    def own_first(mine, other, axis):
        return jnp.where(
            first,
            jnp.concatenate([mine, other], axis=axis),
            jnp.concatenate([other, mine], axis=axis),
        )

    def to_all_y(v):
        sent = jnp.broadcast_to(v[None], (n_y,) + v.shape)
        return lax.all_to_all(sent, "tp", 0, 0, axis_index_groups=y_groups, tiled=True)

    whole = own_first(tokens, lax.ppermute(tokens, "tp", swap), 1)
    ids = expert_ids.T
    named = 2 * jnp.arange(n_ep, dtype=jnp.int32)[:, None] + core
    hit = [(ids[k][None, :] == named) for k in range(top)]
    member = hit[0] | hit[1] | hit[2]
    earlier = (
        jnp.arange(tok, dtype=jnp.int32)[:, None] < jnp.arange(tok, dtype=jnp.int32)[None, :]
    ).astype(BF)
    rank = jnp.dot(member.astype(BF), earlier, preferred_element_type=F32)
    rank = jnp.where(member, rank, -1.0)
    slot_no = jnp.arange(cap, dtype=jnp.int32).astype(F32)
    pick = rank[:, None, :] == slot_no[None, :, None]
    one_hot = pick.astype(BF).reshape(slots, tok)
    outgoing = jnp.dot(one_hot, whole, preferred_element_type=F32).astype(BF)
    arrived = lax.all_to_all(outgoing.reshape(n_ep, cap, width), "ep", 0, 0, tiled=True)
    arrived = arrived.reshape(slots, width)

    gain = own_first(pre_gain, lax.ppermute(after(pre_gain, outgoing), "tp", swap), 0)
    own_rows = lax.dynamic_slice_in_dim(whole, core * half, half, 0)

    sent_in = pack(after(place, outgoing), [expert_gate, expert_up, shared_gate, shared_up])
    got_in = lax.ppermute(sent_in, "tp", swap)
    sent_out = pack(after(place, outgoing), [expert_down, shared_down])
    got_out = lax.ppermute(sent_out, "tp", swap)
    e_down, s_down = expert_down, shared_down
    down_w = own_first(
        lax.dynamic_index_in_dim(e_down, core, 0, keepdims=False), got_out[:n_hid], 1
    ).reshape(n_y, 2 * hid, width)
    sdown_w = own_first(s_down, got_out[n_hid:], 1).reshape(n_y, 2 * hid, width)

    rows = slots + half
    n_sub = rows // 2
    raw = jnp.concatenate([arrived, own_rows], axis=0).astype(F32)
    chunk = (raw * gain).astype(BF)
    square = jnp.sum(raw * raw, axis=1)
    spans = (((0, n_sub, 0),), ((0, slots - n_sub, 0), (slots - n_sub, n_sub, 1)))
    fwd = [chunk[:n_sub], chunk[n_sub:]]
    bwd = list(fwd)
    early, early_at = list(fwd), [(0, 0), (1, 0)]
    late, late_at = [], []
    for step in range(1, n_y // 2 + 1):
        last = step == n_y // 2
        pieces, at = (late, late_at) if last else (early, early_at)
        for k in range(2):
            if not last or k == 0:
                fwd[k] = lax.ppermute(fwd[k], "tp", y_shift(1))
                pieces.append(fwd[k])
                at.append((k, -step))
            if not last or k == 1:
                bwd[k] = lax.ppermute(bwd[k], "tp", y_shift(-1))
                pieces.append(bwd[k])
                at.append((k, step))
        if step == 1:
            squares = to_all_y(after(square, fwd[0]))
        if step == 3:
            square_sum = jnp.sum(after(squares, fwd[0], bwd[0]), axis=0)
            scale = lax.rsqrt(square_sum / feat_all + EPSILON)[:, None]

    flops = 2 * rows * feat_all * 4 * hid
    n_early = len(early)
    total, w_last, sw_last = pl.pallas_call(
        functools.partial(early_kernel, early_at, spans, n_y, width),
        out_shape=(
            jax.ShapeDtypeStruct((rows, 4 * hid), F32),
            jax.ShapeDtypeStruct((4 * hid, width), BF),
            jax.ShapeDtypeStruct((4 * hid, width), BF),
        ),
        in_specs=[SMEM] + [HBM] * (5 + n_early),
        out_specs=(VMEM, VMEM, VMEM),
        scratch_shapes=[
            pltpu.VMEM((4 * hid, feat_all), BF),
            pltpu.VMEM((4 * hid, feat_all), BF),
            pltpu.VMEM((n_early, n_sub, width), BF),
            pltpu.SemaphoreType.DMA((8,)),
            pltpu.SemaphoreType.DMA((n_early,)),
        ],
        cost_estimate=pl.CostEstimate(flops=flops, bytes_accessed=2**23, transcendentals=0),
        compiler_params=pltpu.CompilerParams(vmem_limit_bytes=20 * 2**20),
    )(place, expert_gate, expert_up, shared_gate, shared_up, got_in, *early)
    hidden = pl.pallas_call(
        functools.partial(late_kernel, spans),
        out_shape=jax.ShapeDtypeStruct((n_y, rows, 2 * hid), BF),
        in_specs=[VMEM] * 6,
        out_specs=VMEM,
        cost_estimate=pl.CostEstimate(flops=flops // 8, bytes_accessed=2**21, transcendentals=0),
        compiler_params=pltpu.CompilerParams(vmem_limit_bytes=12 * 2**20),
    )(w_last, sw_last, total, scale, *late)

    hidden_all = lax.all_to_all(hidden, "tp", 0, 0, axis_index_groups=y_groups, tiled=True)
    contract = (((0, 2), (0, 1)), ((), ()))
    expert_out = lax.dot_general(hidden_all[:, :slots], down_w, contract, preferred_element_type=F32).astype(BF)
    returned = lax.all_to_all(expert_out.reshape(n_ep, cap, width), "ep", 0, 0, tiled=True)
    returned = returned.reshape(slots, width)

    shared_out = lax.dot_general(hidden_all[:, slots:], sdown_w, contract, preferred_element_type=F32)
    weight = sum(jnp.where(hit[k], route_weight.T[k][None, :], 0.0) for k in range(top))
    mix = jnp.where(pick, weight[:, None, :], 0.0).reshape(slots, tok)
    high = lax.reduce_precision(mix, 8, 7)
    middle = lax.reduce_precision(mix - high, 8, 7)
    low = mix - high - middle
    part = sum(
        lax.dot_general(m.astype(BF), returned, (((0,), (0,)), ((), ())), preferred_element_type=F32)
        for m in (high, middle, low)
    )
    zero = jnp.zeros_like(shared_out)
    part = part + jnp.where(
        first,
        jnp.concatenate([shared_out, zero], axis=0),
        jnp.concatenate([zero, shared_out], axis=0),
    )
    away = jnp.where(first, part[:, feat:], part[:, :feat])
    home = jnp.where(first, part[:, :feat], part[:, feat:])
    summed = home + lax.ppermute(away, "tp", swap)
    own_square = jnp.sum(summed * summed, axis=1)
    sent = jnp.broadcast_to(own_square[None, :], (n_tp, tok))
    out_square = jnp.sum(lax.all_to_all(sent, "tp", 0, 0, tiled=True), axis=0)
    return (summed * lax.rsqrt(out_square[:, None] / feat_all + EPSILON) * out_gain).astype(BF)


def solution(mesh):
    return jax.shard_map(
        body,
        mesh=mesh,
        in_specs=(
            P("ep", "tp"),
            P("tp"),
            P("ep", None),
            P("ep", None),
            P("ep", "tp", None),
            P("ep", "tp", None),
            P("ep", None, "tp"),
            P("tp", None),
            P("tp", None),
            P(None, "tp"),
            P("tp"),
        ),
        out_specs=P("ep", "tp"),
        check_vma=False,
    )
```

```python
import functools

import jax
import jax.numpy as jnp
from jax import lax
from jax.experimental import pallas as pl
from jax.experimental.pallas import tpu as pltpu
from jax.sharding import PartitionSpec as P


EPSILON = 1e-06
BF = jnp.bfloat16
F32 = jnp.float32


VMEM = pl.BlockSpec(memory_space=pltpu.VMEM)
SMEM = pl.BlockSpec(memory_space=pltpu.SMEM)
HBM = pl.BlockSpec(memory_space=pltpu.HBM)


def times(x, w):
    return lax.dot_general(x, w, (((1,), (1,)), ((), ())), preferred_element_type=F32)


def early_kernel(places, n_y, width, at_ref, gate, up, s_gate, s_up, got, *refs):
    n, ns = len(places), n_y
    pieces, shared = refs[:n], refs[n : n + ns]
    total_ref, s_total_ref, w_last = refs[n + ns : n + ns + 3]
    w, sw, held, s_held, w_sem, sem, s_sem = refs[n + ns + 3 :]
    core, y = at_ref[0], at_ref[1]
    hid = s_gate.shape[0]
    n_sub = total_ref.shape[0] // 2
    own = pl.multiple_of(core * hid, hid)
    other = pl.multiple_of((1 - core) * hid, hid)

    def columns(offset):
        return pl.ds(pl.multiple_of(lax.rem(y + offset + n_y, n_y) * width, width), width)

    moves = []
    for i, (mine, into, base) in enumerate(
        ((gate.at[core], w, 0), (up.at[core], w, 2 * hid), (s_gate, sw, 0), (s_up, sw, 2 * hid))
    ):
        moves.append(pltpu.make_async_copy(mine, into.at[pl.ds(base + own, hid)], w_sem.at[2 * i]))
        theirs = got.at[pl.ds(i * hid, hid)]
        moves.append(pltpu.make_async_copy(theirs, into.at[pl.ds(base + other, hid)], w_sem.at[2 * i + 1]))
    loads = [
        pltpu.make_async_copy(p, held.at[pl.ds(k * n_sub, n_sub), columns(offset)], sem.at[i])
        for i, (p, (k, offset)) in enumerate(zip(pieces, places))
    ]
    s_loads = [
        pltpu.make_async_copy(p, s_held.at[:, columns(offset)], s_sem.at[i])
        for i, (p, offset) in enumerate(zip(shared, shared_offsets(n_y)))
    ]
    for copy in moves[:4] + loads + moves[4:] + s_loads:
        copy.start()
    held[:, columns(n_y // 2)] = jnp.zeros((2 * n_sub, width), BF)
    for copy in moves[:4] + loads:
        copy.wait()
    total_ref[...] = times(held[...], w[...])
    w_last[...] = w[:, columns(n_y // 2)]
    for copy in moves[4:] + s_loads:
        copy.wait()
    s_total_ref[...] = times(s_held[...], sw[...])


def shared_offsets(n_y):
    steps = range(1, n_y // 2 + 1)
    return [0] + [o for s in steps for o in ((-s, s) if s < n_y // 2 else (-s,))]


def late_kernel(w_ref, total_ref, s_total_ref, scale_ref, *refs):
    out_ref = refs[-1]
    n = total_ref.shape[0]
    n_sub = n // 2
    for half in range(2):
        rows = slice(half * n_sub, (half + 1) * n_sub)
        total = total_ref[rows, :] + times(refs[half][...], w_ref[...])
        hidden = activated(total * scale_ref[rows, :])
        for j in range(out_ref.shape[0]):
            out_ref[j, rows, :] = hidden
    hidden = activated(s_total_ref[...] * scale_ref[n:, :])
    for j in range(out_ref.shape[0]):
        out_ref[j, n:, :] = hidden


def activated(total):
    n = total.shape[1] // 2
    gate, up = total[:, :n], total[:, n:]
    return (gate / (1.0 + jnp.exp(-gate)) * up).astype(BF)


def pack_kernel(at_ref, *refs):
    n = len(refs) - 3
    arrays, out_ref, held, sem = refs[:n], refs[n], refs[n + 1], refs[n + 2]
    rows = out_ref.shape[0] // n
    ins = []
    for i, a in enumerate(arrays):
        part = a.at[1 - at_ref[0]] if len(a.shape) == 3 else a
        ins.append(pltpu.make_async_copy(part, held.at[pl.ds(i * rows, rows)], sem.at[i]))
    outs = [
        pltpu.make_async_copy(
            held.at[pl.ds(i * rows, rows)], out_ref.at[pl.ds(i * rows, rows)], sem.at[n + i]
        )
        for i in range(n)
    ]
    for copy in ins:
        copy.start()
    for i in range(n):
        ins[i].wait()
        outs[i].start()
    for copy in outs:
        copy.wait()


def pack(at, arrays):
    rows, cols = arrays[0].shape[-2:]
    shape = (rows * len(arrays), cols)
    return pl.pallas_call(
        pack_kernel,
        out_shape=jax.ShapeDtypeStruct(shape, BF),
        in_specs=[SMEM] + [HBM] * len(arrays),
        out_specs=HBM,
        scratch_shapes=[pltpu.VMEM(shape, BF), pltpu.SemaphoreType.DMA((2 * len(arrays),))],
        cost_estimate=pl.CostEstimate(flops=4 * 10**8, bytes_accessed=2**22, transcendentals=0),
        compiler_params=pltpu.CompilerParams(vmem_limit_bytes=4 * 2**20),
    )(at, *arrays)


def body(
    tokens,
    pre_gain,
    expert_ids,
    route_weight,
    expert_gate,
    expert_up,
    expert_down,
    shared_gate,
    shared_up,
    shared_down,
    out_gain,
):
    tok, top = expert_ids.shape
    n_ep = lax.axis_size("ep")
    n_tp = lax.axis_size("tp")
    n_y = n_tp // 2
    experts = expert_gate.shape[0] * n_ep
    cap = 4 * tok * top // (3 * experts)
    feat = tokens.shape[1]
    feat_all = feat * n_tp
    width = 2 * feat
    hid = expert_gate.shape[1]
    n_hid = expert_down.shape[1]
    half = tok // 2
    slots = n_ep * cap
    tp = lax.axis_index("tp")
    core = lax.rem(tp, 2)
    y = lax.div(tp, 2)
    first = core == 0

    place = jnp.stack([core, y]).astype(jnp.int32)
    swap = [(i, i ^ 1) for i in range(n_tp)]
    y_groups = [[c + 2 * k for k in range(n_y)] for c in range(2)]

    def y_shift(d):
        return [(i, ((i // 2 + d) % n_y) * 2 + i % 2) for i in range(n_tp)]

    def own_first(mine, other, axis):
        return jnp.where(
            first,
            jnp.concatenate([mine, other], axis=axis),
            jnp.concatenate([other, mine], axis=axis),
        )

    def to_all_y(v):
        sent = jnp.broadcast_to(v[None], (n_y,) + v.shape)
        return lax.all_to_all(sent, "tp", 0, 0, axis_index_groups=y_groups, tiled=True)

    g_high = lax.reduce_precision(pre_gain, 8, 7)
    g_middle = lax.reduce_precision(pre_gain - g_high, 8, 7)
    g_rows = jnp.stack([g_high, g_middle, pre_gain - g_high - g_middle] + [jnp.zeros_like(g_high)] * 13)
    partner = lax.ppermute(jnp.concatenate([tokens, g_rows.astype(BF)], axis=0), "tp", swap)
    whole = own_first(tokens, partner[:tok], 1)
    partner_gain = jnp.sum(partner[tok : tok + 3].astype(F32), axis=0)
    gain = own_first(pre_gain, partner_gain, 0)
    ids = expert_ids.T
    named = 2 * jnp.arange(n_ep, dtype=jnp.int32)[:, None] + core
    hit = [(ids[k][None, :] == named) for k in range(top)]
    member = hit[0] | hit[1] | hit[2]
    earlier = (
        jnp.arange(tok, dtype=jnp.int32)[:, None] < jnp.arange(tok, dtype=jnp.int32)[None, :]
    ).astype(BF)
    rank = jnp.dot(member.astype(BF), earlier, preferred_element_type=F32)
    rank = jnp.where(member, rank, -1.0)
    slot_no = jnp.arange(cap, dtype=jnp.int32).astype(F32)
    pick = rank[:, None, :] == slot_no[None, :, None]
    one_hot = pick.astype(BF).reshape(slots, tok)
    outgoing = jnp.dot(one_hot, whole, preferred_element_type=F32).astype(BF)
    arrived = lax.all_to_all(outgoing.reshape(n_ep, cap, width), "ep", 0, 0, tiled=True)
    arrived = arrived.reshape(slots, width)

    own_rows = lax.dynamic_slice_in_dim(whole, core * half, half, 0)
    shared = [(own_rows.astype(F32) * gain).astype(BF)]
    s_fwd = s_bwd = shared[0]

    def shared_step(step):
        f, b = s_fwd, s_bwd
        f = lax.ppermute(f, "tp", y_shift(1))
        shared.append(f)
        if step < n_y // 2:
            b = lax.ppermute(b, "tp", y_shift(-1))
            shared.append(b)
        return f, b

    s_fwd, s_bwd = shared_step(1)
    s_fwd, s_bwd = shared_step(2)

    sent_out = pack(place, [expert_down, shared_down])
    got_out = lax.ppermute(sent_out, "tp", swap)
    e_down, s_down = expert_down, shared_down
    down_w = own_first(
        lax.dynamic_index_in_dim(e_down, core, 0, keepdims=False), got_out[:n_hid], 1
    ).reshape(n_y, 2 * hid, width)
    sdown_w = own_first(s_down, got_out[n_hid:], 1).reshape(n_y, 2 * hid, width)

    rows = slots + half
    n_sub = slots // 2
    arrived, shared[1], shared[2] = lax.optimization_barrier((arrived, shared[1], shared[2]))
    raw = arrived.astype(F32)
    chunk = (raw * gain).astype(BF)
    own_rows = own_rows.astype(F32)
    square = jnp.concatenate([jnp.sum(raw * raw, axis=1), jnp.sum(own_rows * own_rows, axis=1)])
    fwd = [chunk[:n_sub], chunk[n_sub:]]
    bwd = list(fwd)
    early, early_at = list(fwd), [(0, 0), (1, 0)]
    late, late_at = [], []
    for step in range(1, n_y // 2 + 1):
        last = step == n_y // 2
        pieces, at = (late, late_at) if last else (early, early_at)
        for k in range(2):
            if not last or k == 0:
                fwd[k] = lax.ppermute(fwd[k], "tp", y_shift(1))
                pieces.append(fwd[k])
                at.append((k, -step))
            if not last or k == 1:
                bwd[k] = lax.ppermute(bwd[k], "tp", y_shift(-1))
                pieces.append(bwd[k])
                at.append((k, step))
        if step == 1:
            squares = to_all_y(square)
            sent_in = pack(
                place, [expert_gate, expert_up, shared_gate, shared_up]
            )
            got_in = lax.ppermute(sent_in, "tp", swap)
            s_fwd, s_bwd = shared_step(3)
        if step == 2:
            s_fwd, s_bwd = shared_step(4)
        if step == 3:
            square_sum = jnp.sum(squares, axis=0)
            scale = lax.rsqrt(square_sum / feat_all + EPSILON)[:, None]

    flops = 2 * rows * feat_all * 4 * hid
    n_early = len(early)
    total, s_total, w_last = pl.pallas_call(
        functools.partial(early_kernel, early_at, n_y, width),
        out_shape=(
            jax.ShapeDtypeStruct((slots, 4 * hid), F32),
            jax.ShapeDtypeStruct((half, 4 * hid), F32),
            jax.ShapeDtypeStruct((4 * hid, width), BF),
        ),
        in_specs=[SMEM] + [HBM] * (5 + n_early + n_y),
        out_specs=(VMEM, VMEM, VMEM),
        scratch_shapes=[
            pltpu.VMEM((4 * hid, feat_all), BF),
            pltpu.VMEM((4 * hid, feat_all), BF),
            pltpu.VMEM((slots, feat_all), BF),
            pltpu.VMEM((half, feat_all), BF),
            pltpu.SemaphoreType.DMA((8,)),
            pltpu.SemaphoreType.DMA((n_early,)),
            pltpu.SemaphoreType.DMA((n_y,)),
        ],
        cost_estimate=pl.CostEstimate(flops=flops, bytes_accessed=2**23, transcendentals=0),
        compiler_params=pltpu.CompilerParams(vmem_limit_bytes=24 * 2**20),
    )(place, expert_gate, expert_up, shared_gate, shared_up, got_in, *early, *shared)
    hidden = pl.pallas_call(
        late_kernel,
        out_shape=jax.ShapeDtypeStruct((n_y, rows, 2 * hid), BF),
        in_specs=[VMEM] * 6,
        out_specs=VMEM,
        cost_estimate=pl.CostEstimate(flops=flops // 8, bytes_accessed=2**21, transcendentals=0),
        compiler_params=pltpu.CompilerParams(vmem_limit_bytes=12 * 2**20),
    )(w_last, total, s_total, scale, *late)

    hidden_all = lax.all_to_all(hidden, "tp", 0, 0, axis_index_groups=y_groups, tiled=True)
    contract = (((0, 2), (0, 1)), ((), ()))
    expert_out = lax.dot_general(hidden_all[:, :slots], down_w, contract, preferred_element_type=F32).astype(BF)
    returned = lax.all_to_all(expert_out.reshape(n_ep, cap, width), "ep", 0, 0, tiled=True)
    returned = returned.reshape(slots, width)

    shared_out = lax.dot_general(hidden_all[:, slots:], sdown_w, contract, preferred_element_type=F32)
    weight = sum(jnp.where(hit[k], route_weight.T[k][None, :], 0.0) for k in range(top))
    mix = jnp.where(pick, weight[:, None, :], 0.0).reshape(slots, tok)
    high = lax.reduce_precision(mix, 8, 7)
    middle = lax.reduce_precision(mix - high, 8, 7)
    low = mix - high - middle
    part = sum(
        lax.dot_general(m.astype(BF), returned, (((0,), (0,)), ((), ())), preferred_element_type=F32)
        for m in (high, middle, low)
    )
    zero = jnp.zeros_like(shared_out)
    part = part + jnp.where(
        first,
        jnp.concatenate([shared_out, zero], axis=0),
        jnp.concatenate([zero, shared_out], axis=0),
    )
    away = jnp.where(first, part[:, feat:], part[:, :feat])
    home = jnp.where(first, part[:, :feat], part[:, feat:])
    summed = home + lax.ppermute(away, "tp", swap)
    own_square = jnp.sum(summed * summed, axis=1)
    sent = jnp.broadcast_to(own_square[None, :], (n_tp, tok))
    out_square = jnp.sum(lax.all_to_all(sent, "tp", 0, 0, tiled=True), axis=0)
    return (summed * lax.rsqrt(out_square[:, None] / feat_all + EPSILON) * out_gain).astype(BF)


def solution(mesh):
    return jax.shard_map(
        body,
        mesh=mesh,
        in_specs=(
            P("ep", "tp"),
            P("tp"),
            P("ep", None),
            P("ep", None),
            P("ep", "tp", None),
            P("ep", "tp", None),
            P("ep", None, "tp"),
            P("tp", None),
            P("tp", None),
            P(None, "tp"),
            P("tp"),
        ),
        out_specs=P("ep", "tp"),
        check_vma=False,
    )
```

```python
import functools

import jax
import jax.numpy as jnp
from jax import lax
from jax.experimental import pallas as pl
from jax.experimental.pallas import tpu as pltpu
from jax.sharding import PartitionSpec as P


EPSILON = 1e-06
BF = jnp.bfloat16
F32 = jnp.float32
SPARE = 8


VMEM = pl.BlockSpec(memory_space=pltpu.VMEM)
SMEM = pl.BlockSpec(memory_space=pltpu.SMEM)


def times(x, w):
    return lax.dot_general(x, w, (((1,), (1,)), ((), ())), preferred_element_type=F32)


def thirds(v):
    high = v.astype(BF)
    rest = v - high.astype(F32)
    middle = rest.astype(BF)
    return high, middle, (rest - middle.astype(F32)).astype(BF)


def picks(ids, core, n_ep, cap):
    tok = ids.shape[1]
    named = 2 * lax.broadcasted_iota(jnp.int32, (n_ep, tok), 0) + core
    member = ids[0:1, :] == named
    for k in range(1, ids.shape[0]):
        member = member | (ids[k : k + 1, :] == named)
    before = lax.broadcasted_iota(jnp.int32, (tok, tok), 0) < lax.broadcasted_iota(jnp.int32, (tok, tok), 1)
    one = jnp.where(member, 1.0, 0.0).astype(BF)
    rank = jnp.dot(one, jnp.where(before, 1.0, 0.0).astype(BF), preferred_element_type=F32)
    rank = jnp.where(member, rank, -1.0)
    spread = jnp.broadcast_to(rank[:, None, :], (n_ep, cap, tok))
    slot = lax.broadcasted_iota(jnp.int32, (n_ep, cap, tok), 1).astype(F32)
    return jnp.where(spread == slot, 1.0, 0.0).astype(BF).reshape(n_ep * cap, tok)


def route_kernel(n_ep, cap, at_ref, ids_ref, own_ref, other_ref, out_ref):
    core = at_ref[0]
    one_hot = picks(ids_ref[...], core, n_ep, cap)
    feat = own_ref.shape[1]
    for ref, where in ((own_ref, core), (other_ref, 1 - core)):
        at = pl.ds(pl.multiple_of(where * feat, feat), feat)
        out_ref[:, at] = jnp.dot(one_hot, ref[...], preferred_element_type=F32).astype(BF)


def arrive_kernel(at_ref, rows_ref, own_ref, other_ref, gain_ref, first_ref, second_ref):
    core = at_ref[0]
    slots, width = rows_ref.shape
    half, feat = own_ref.shape[0] // 2, own_ref.shape[1]
    n_sub = (slots + half) // 2
    mine = pl.ds(pl.multiple_of(core * half, half), half)
    own, other = own_ref[mine, :], other_ref[mine, :]
    own, other = jnp.where(core == 0, own, other), jnp.where(core == 0, other, own)
    split = slots - n_sub
    gain = gain_ref[...]

    def put(ref, at, rows, columns):
        raw = rows.astype(F32)
        ref[at : at + rows.shape[0], columns] = (raw * gain[:, columns]).astype(BF)
        return raw * raw

    every, left, right = slice(0, width), slice(0, feat), slice(feat, width)

    def total(squares):
        ones = jnp.ones((SPARE, squares.shape[1]), F32)
        return lax.dot_general(
            ones, squares, (((1,), (1,)), ((), ())), precision=lax.Precision.HIGHEST, preferred_element_type=F32
        )

    def spare(ref, at, sums):
        high, middle, low = thirds(sums)
        row = lax.broadcasted_iota(jnp.int32, sums.shape, 0)
        parts = jnp.where(row == 0, high.astype(F32), jnp.where(row == 1, middle.astype(F32), low.astype(F32)))
        ref[n_sub:, at : at + sums.shape[1]] = jnp.where(row < 3, parts, 0.0).astype(BF)

    for ref in (first_ref, second_ref):
        ref[n_sub:, :] = jnp.zeros((SPARE, width), BF)
    spare(first_ref, 0, total(put(first_ref, 0, rows_ref[:n_sub, :], every)))
    sums = total(put(second_ref, 0, rows_ref[n_sub:, :], every))
    tail = total(put(second_ref, split, own, left)) + total(put(second_ref, split, other, right))
    spare(second_ref, 0, jnp.concatenate([sums, tail], axis=1))


def early_kernel(places, spans, n_y, width, at_ref, gate, up, s_gate, s_up, got, *refs):
    n = len(places)
    pieces = refs[:n]
    total_ref, squares_ref, w_last, sw_last, w, sw = refs[n:]
    core, y = at_ref[0], at_ref[1]
    hid = s_gate.shape[0]
    n_sub = total_ref.shape[0] // 2
    own = pl.multiple_of(core * hid, hid)
    other = pl.multiple_of((1 - core) * hid, hid)
    for i, (mine, into, base) in enumerate(
        ((gate.at[core], w, 0), (up.at[core], w, 2 * hid), (s_gate, sw, 0), (s_up, sw, 2 * hid))
    ):
        into[pl.ds(base + own, hid), :] = mine[...]
        into[pl.ds(base + other, hid), :] = got[i * hid : (i + 1) * hid, :]

    def columns(offset):
        return pl.ds(pl.multiple_of(lax.rem(y + offset + n_y, n_y) * width, width), width)

    for half in range(2):
        total = [None] * len(spans[half])
        squares = jnp.zeros((SPARE, width), F32)
        for piece, (k, offset) in zip(pieces, places):
            if k != half:
                continue
            for j, (low, high, which) in enumerate(spans[half]):
                term = times(piece[low:high, :], (w, sw)[which][:, columns(offset)])
                total[j] = term if total[j] is None else total[j] + term
            squares = squares + piece[n_sub:, :].astype(F32)
        for (low, high, _), value in zip(spans[half], total):
            total_ref[half * n_sub + low : half * n_sub + high, :] = value
        squares_ref[half * SPARE : (half + 1) * SPARE, :] = squares
    w_last[...] = w[:, columns(n_y // 2)]
    sw_last[...] = sw[:, columns(n_y // 2)]


def late_kernel(spans, features, w_ref, sw_ref, total_ref, squares_ref, *refs):
    out_ref = refs[-1]
    n_sub = total_ref.shape[0] // 2
    for half in range(2):
        piece = refs[half]
        squares = squares_ref[half * SPARE : (half + 1) * SPARE, :] + piece[n_sub:, :].astype(F32)
        squares = jnp.sum(squares, axis=0, keepdims=True)
        scale = lax.rsqrt(squares / features + EPSILON)
        scale = jnp.broadcast_to(scale, (128, scale.shape[1])).T
        for low, high, which in spans[half]:
            rows = slice(half * n_sub + low, half * n_sub + high)
            total = total_ref[rows, :] + times(piece[low:high, :], (w_ref, sw_ref)[which][...])
            n = total.shape[1] // 2
            gate, up = total[:, :n] * scale[low:high, :n], total[:, n:] * scale[low:high, :n]
            hidden = (gate / (1.0 + jnp.exp(-gate)) * up).astype(BF)
            for j in range(out_ref.shape[0]):
                out_ref[j, rows, :] = hidden


def down_kernel(at_ref, hidden_ref, own_ref, got_ref, out_ref):
    core = at_ref[0]
    feat = own_ref.shape[2]
    slots = out_ref.shape[0]
    hidden = jnp.concatenate([hidden_ref[j, :slots, :] for j in range(hidden_ref.shape[0])], axis=1)
    for w, where in ((own_ref.at[core], core), (got_ref, 1 - core)):
        at = pl.ds(pl.multiple_of(where * feat, feat), feat)
        out_ref[:, at] = jnp.dot(
            hidden, w[: hidden.shape[1], :], preferred_element_type=F32
        ).astype(BF)


def pack_kernel(at_ref, *refs):
    arrays, out_ref = refs[:-1], refs[-1]
    rows = out_ref.shape[0] // len(arrays)
    for i, a in enumerate(arrays):
        part = a.at[1 - at_ref[0]] if len(a.shape) == 3 else a
        out_ref[i * rows : (i + 1) * rows, :] = part[...]


def call(kernel, out, args, flops, mib, scratch=()):
    return pl.pallas_call(
        kernel,
        out_shape=out,
        in_specs=[SMEM] + [VMEM] * (len(args) - 1),
        out_specs=jax.tree.map(lambda _: VMEM, out),
        scratch_shapes=scratch,
        cost_estimate=pl.CostEstimate(flops=flops, bytes_accessed=2**21, transcendentals=0),
        compiler_params=pltpu.CompilerParams(vmem_limit_bytes=mib * 2**20),
    )(*args)


def body(
    tokens,
    pre_gain,
    expert_ids,
    route_weight,
    expert_gate,
    expert_up,
    expert_down,
    shared_gate,
    shared_up,
    shared_down,
    out_gain,
):
    tok, top = expert_ids.shape
    n_ep = lax.axis_size("ep")
    n_tp = lax.axis_size("tp")
    n_y = n_tp // 2
    experts = expert_gate.shape[0] * n_ep
    cap = 4 * tok * top // (3 * experts)
    feat = tokens.shape[1]
    feat_all = feat * n_tp
    width = 2 * feat
    hid = expert_gate.shape[1]
    n_hid = expert_down.shape[1]
    half = tok // 2
    slots = n_ep * cap
    rows = slots + half
    n_sub = rows // 2
    tp = lax.axis_index("tp")
    core = lax.rem(tp, 2)
    y = lax.div(tp, 2)
    first = core == 0
    place = jnp.stack([core, y]).astype(jnp.int32)

    swap = [(i, i ^ 1) for i in range(n_tp)]
    y_groups = [[c + 2 * k for k in range(n_y)] for c in range(2)]

    def y_shift(d):
        return [(i, ((i // 2 + d) % n_y) * 2 + i % 2) for i in range(n_tp)]

    def own_first(mine, other, axis):
        return jnp.where(
            first,
            jnp.concatenate([mine, other], axis=axis),
            jnp.concatenate([other, mine], axis=axis),
        )

    partner = lax.ppermute(tokens, "tp", swap)
    ids = expert_ids.T
    outgoing = call(
        functools.partial(route_kernel, n_ep, cap),
        jax.ShapeDtypeStruct((slots, width), BF),
        (place, ids, tokens, partner),
        10**8,
        8,
    )
    arrived = lax.all_to_all(outgoing.reshape(n_ep, cap, width), "ep", 0, 0, tiled=True)
    arrived = arrived.reshape(slots, width)

    gain = own_first(pre_gain, lax.ppermute(pre_gain, "tp", swap), 0)[None, :]
    sent_in = call(
        pack_kernel,
        jax.ShapeDtypeStruct((4 * hid, feat_all), BF),
        (place, expert_gate, expert_up, shared_gate, shared_up),
        4 * 10**8,
        8,
    )
    got_in = lax.ppermute(sent_in, "tp", swap)
    sent_out = call(
        pack_kernel,
        jax.ShapeDtypeStruct((2 * n_hid, feat), BF),
        (place, expert_down, shared_down),
        4 * 10**8,
        6,
    )
    got_out = lax.ppermute(sent_out, "tp", swap)

    piece = jax.ShapeDtypeStruct((n_sub + SPARE, width), BF)
    fwd = call(arrive_kernel, (piece, piece), (place, arrived, tokens, partner, gain), 4 * 10**8, 8)
    fwd, bwd = list(fwd), list(fwd)
    spans = (((0, n_sub, 0),), ((0, slots - n_sub, 0), (slots - n_sub, n_sub, 1)))
    early, early_at = list(fwd), [(0, 0), (1, 0)]
    late, late_at = [], []
    for step in range(1, n_y // 2 + 1):
        last = step == n_y // 2
        pieces, at = (late, late_at) if last else (early, early_at)
        for k in range(2):
            if not last or k == 0:
                fwd[k] = lax.ppermute(fwd[k], "tp", y_shift(1))
                pieces.append(fwd[k])
                at.append((k, -step))
            if not last or k == 1:
                bwd[k] = lax.ppermute(bwd[k], "tp", y_shift(-1))
                pieces.append(bwd[k])
                at.append((k, step))

    flops = 2 * rows * feat_all * 4 * hid
    total, squares, w_last, sw_last = call(
        functools.partial(early_kernel, early_at, spans, n_y, width),
        (
            jax.ShapeDtypeStruct((rows, 4 * hid), F32),
            jax.ShapeDtypeStruct((2 * SPARE, width), F32),
            jax.ShapeDtypeStruct((4 * hid, width), BF),
            jax.ShapeDtypeStruct((4 * hid, width), BF),
        ),
        (place, expert_gate, expert_up, shared_gate, shared_up, got_in, *early),
        flops,
        20,
        [pltpu.VMEM((4 * hid, feat_all), BF), pltpu.VMEM((4 * hid, feat_all), BF)],
    )
    hidden = call(
        lambda _, *refs: late_kernel(spans, feat_all, *refs),
        jax.ShapeDtypeStruct((n_y, rows, 2 * hid), BF),
        (place, w_last, sw_last, total, squares, *late),
        flops // 8,
        8,
    )

    hidden_all = lax.all_to_all(hidden, "tp", 0, 0, axis_index_groups=y_groups, tiled=True)
    expert_out = call(
        down_kernel,
        jax.ShapeDtypeStruct((slots, width), BF),
        (place, hidden_all, expert_down, got_out),
        2 * slots * n_hid * width,
        12,
    )
    returned = lax.all_to_all(expert_out.reshape(n_ep, cap, width), "ep", 0, 0, tiled=True)
    returned = returned.reshape(slots, width)

    sdown_w = own_first(shared_down, got_out[n_hid:], 1).reshape(n_y, 2 * hid, width)
    contract = (((0, 2), (0, 1)), ((), ()))
    shared_out = lax.dot_general(hidden_all[:, slots:], sdown_w, contract, preferred_element_type=F32)
    named = 2 * jnp.arange(n_ep, dtype=jnp.int32)[:, None] + core
    hit = [(ids[k][None, :] == named) for k in range(top)]
    member = hit[0] | hit[1] | hit[2]
    earlier = (
        jnp.arange(tok, dtype=jnp.int32)[:, None] < jnp.arange(tok, dtype=jnp.int32)[None, :]
    ).astype(BF)
    rank = jnp.dot(member.astype(BF), earlier, preferred_element_type=F32)
    rank = jnp.where(member, rank, -1.0)
    slot_no = jnp.arange(cap, dtype=jnp.int32).astype(F32)
    pick = rank[:, None, :] == slot_no[None, :, None]
    weight = sum(jnp.where(hit[k], route_weight.T[k][None, :], 0.0) for k in range(top))
    mix = jnp.where(pick, weight[:, None, :], 0.0).reshape(slots, tok)
    high = lax.reduce_precision(mix, 8, 7)
    middle = lax.reduce_precision(mix - high, 8, 7)
    low = mix - high - middle
    part = sum(
        lax.dot_general(m.astype(BF), returned, (((0,), (0,)), ((), ())), preferred_element_type=F32)
        for m in (high, middle, low)
    )
    zero = jnp.zeros_like(shared_out)
    part = part + jnp.where(
        first,
        jnp.concatenate([shared_out, zero], axis=0),
        jnp.concatenate([zero, shared_out], axis=0),
    )
    away = jnp.where(first, part[:, feat:], part[:, :feat])
    home = jnp.where(first, part[:, :feat], part[:, feat:])
    summed = home + lax.ppermute(away, "tp", swap)
    own_square = jnp.sum(summed * summed, axis=1)
    sent = jnp.broadcast_to(own_square[None, :], (n_tp, tok))
    out_square = jnp.sum(lax.all_to_all(sent, "tp", 0, 0, tiled=True), axis=0)
    return (summed * lax.rsqrt(out_square[:, None] / feat_all + EPSILON) * out_gain).astype(BF)


def solution(mesh):
    return jax.shard_map(
        body,
        mesh=mesh,
        in_specs=(
            P("ep", "tp"),
            P("tp"),
            P("ep", None),
            P("ep", None),
            P("ep", "tp", None),
            P("ep", "tp", None),
            P("ep", None, "tp"),
            P("tp", None),
            P("tp", None),
            P(None, "tp"),
            P("tp"),
        ),
        out_specs=P("ep", "tp"),
        check_vma=False,
    )
```

```python
import functools

import jax
import jax.numpy as jnp
from jax import lax
from jax.experimental import pallas as pl
from jax.experimental.pallas import tpu as pltpu
from jax.sharding import PartitionSpec as P


EPSILON = 1e-06
BF = jnp.bfloat16
F32 = jnp.float32
SPARE = 8


VMEM = pl.BlockSpec(memory_space=pltpu.VMEM)
SMEM = pl.BlockSpec(memory_space=pltpu.SMEM)


def times(x, w):
    return lax.dot_general(x, w, (((1,), (1,)), ((), ())), preferred_element_type=F32)


def thirds(v):
    high = v.astype(BF)
    rest = v - high.astype(F32)
    middle = rest.astype(BF)
    return high, middle, (rest - middle.astype(F32)).astype(BF)


def picks(ids, core, n_ep, cap, weight=None):
    tok = ids.shape[1]
    named = 2 * lax.broadcasted_iota(jnp.int32, (n_ep, tok), 0) + core
    member = ids[0:1, :] == named
    for k in range(1, ids.shape[0]):
        member = member | (ids[k : k + 1, :] == named)
    before = lax.broadcasted_iota(jnp.int32, (tok, tok), 0) < lax.broadcasted_iota(jnp.int32, (tok, tok), 1)
    one = jnp.where(member, 1.0, 0.0).astype(BF)
    rank = jnp.dot(one, jnp.where(before, 1.0, 0.0).astype(BF), preferred_element_type=F32)
    rank = jnp.where(member, rank, -1.0)
    spread = jnp.broadcast_to(rank[:, None, :], (n_ep, cap, tok))
    slot = lax.broadcasted_iota(jnp.int32, (n_ep, cap, tok), 1).astype(F32)
    if weight is None:
        return jnp.where(spread == slot, 1.0, 0.0).astype(BF).reshape(n_ep * cap, tok)
    value = jnp.where(ids[0:1, :] == named, weight[0:1, :], 0.0)
    for k in range(1, ids.shape[0]):
        value = value + jnp.where(ids[k : k + 1, :] == named, weight[k : k + 1, :], 0.0)
    value = jnp.broadcast_to(value[:, None, :], (n_ep, cap, tok))
    return jnp.where(spread == slot, value, 0.0).reshape(n_ep * cap, tok)


def mix_kernel(n_ep, cap, at_ref, ids_ref, weight_ref, *out_refs):
    mix = picks(ids_ref[...], at_ref[0], n_ep, cap, weight_ref[...]).T
    for ref, value in zip(out_refs, thirds(mix)):
        ref[...] = value


def combine_kernel(at_ref, high, middle, low, rows_ref, shared_ref, home_ref, away_ref):
    core = at_ref[0]
    rows = rows_ref[...]
    part = jnp.dot(high[...], rows, preferred_element_type=F32)
    part = part + jnp.dot(middle[...], rows, preferred_element_type=F32)
    part = part + jnp.dot(low[...], rows, preferred_element_type=F32)
    shared = shared_ref[...]
    half, feat = shared.shape[0], home_ref.shape[1]
    top = part[:half] + jnp.where(core == 0, shared, 0.0)
    bottom = part[half:] + jnp.where(core == 0, 0.0, shared)
    for at, value in ((slice(0, half), top), (slice(half, 2 * half), bottom)):
        left, right = value[:, :feat], value[:, feat:]
        home_ref[at, :] = jnp.where(core == 0, left, right)
        away_ref[at, :] = jnp.where(core == 0, right, left)


def route_kernel(n_ep, cap, at_ref, ids_ref, own_ref, other_ref, out_ref):
    core = at_ref[0]
    one_hot = picks(ids_ref[...], core, n_ep, cap)
    feat = own_ref.shape[1]
    for ref, where in ((own_ref, core), (other_ref, 1 - core)):
        at = pl.ds(pl.multiple_of(where * feat, feat), feat)
        out_ref[:, at] = jnp.dot(one_hot, ref[...], preferred_element_type=F32).astype(BF)


def arrive_kernel(at_ref, rows_ref, own_ref, other_ref, gain_ref, first_ref, second_ref):
    core = at_ref[0]
    slots, width = rows_ref.shape
    half, feat = own_ref.shape[0] // 2, own_ref.shape[1]
    n_sub = (slots + half) // 2
    mine = pl.ds(pl.multiple_of(core * half, half), half)
    own, other = own_ref[mine, :], other_ref[mine, :]
    own, other = jnp.where(core == 0, own, other), jnp.where(core == 0, other, own)
    split = slots - n_sub
    gain = gain_ref[...]

    def put(ref, at, rows, columns):
        raw = rows.astype(F32)
        ref[at : at + rows.shape[0], columns] = (raw * gain[:, columns]).astype(BF)
        return raw * raw

    every, left, right = slice(0, width), slice(0, feat), slice(feat, width)

    def total(squares):
        ones = jnp.ones((SPARE, squares.shape[1]), F32)
        return lax.dot_general(
            ones, squares, (((1,), (1,)), ((), ())), precision=lax.Precision.HIGHEST, preferred_element_type=F32
        )

    def spare(ref, at, sums):
        high, middle, low = thirds(sums)
        row = lax.broadcasted_iota(jnp.int32, sums.shape, 0)
        parts = jnp.where(row == 0, high.astype(F32), jnp.where(row == 1, middle.astype(F32), low.astype(F32)))
        ref[n_sub:, at : at + sums.shape[1]] = jnp.where(row < 3, parts, 0.0).astype(BF)

    for ref in (first_ref, second_ref):
        ref[n_sub:, :] = jnp.zeros((SPARE, width), BF)
    spare(first_ref, 0, total(put(first_ref, 0, rows_ref[:n_sub, :], every)))
    sums = total(put(second_ref, 0, rows_ref[n_sub:, :], every))
    tail = total(put(second_ref, split, own, left)) + total(put(second_ref, split, other, right))
    spare(second_ref, 0, jnp.concatenate([sums, tail], axis=1))


def early_kernel(places, spans, n_y, width, at_ref, gate, up, s_gate, s_up, got, *refs):
    n = len(places)
    pieces = refs[:n]
    total_ref, squares_ref, w_last, sw_last, w, sw = refs[n:]
    core, y = at_ref[0], at_ref[1]
    hid = s_gate.shape[0]
    n_sub = total_ref.shape[0] // 2
    own = pl.multiple_of(core * hid, hid)
    other = pl.multiple_of((1 - core) * hid, hid)
    for i, (mine, into, base) in enumerate(
        ((gate.at[core], w, 0), (up.at[core], w, 2 * hid), (s_gate, sw, 0), (s_up, sw, 2 * hid))
    ):
        into[pl.ds(base + own, hid), :] = mine[...]
        into[pl.ds(base + other, hid), :] = got[i * hid : (i + 1) * hid, :]

    def columns(offset):
        return pl.ds(pl.multiple_of(lax.rem(y + offset + n_y, n_y) * width, width), width)

    for half in range(2):
        total = [None] * len(spans[half])
        squares = jnp.zeros((SPARE, width), F32)
        for piece, (k, offset) in zip(pieces, places):
            if k != half:
                continue
            for j, (low, high, which) in enumerate(spans[half]):
                term = times(piece[low:high, :], (w, sw)[which][:, columns(offset)])
                total[j] = term if total[j] is None else total[j] + term
            squares = squares + piece[n_sub:, :].astype(F32)
        for (low, high, _), value in zip(spans[half], total):
            total_ref[half * n_sub + low : half * n_sub + high, :] = value
        squares_ref[half * SPARE : (half + 1) * SPARE, :] = squares
    w_last[...] = w[:, columns(n_y // 2)]
    sw_last[...] = sw[:, columns(n_y // 2)]


def late_kernel(spans, features, w_ref, sw_ref, total_ref, squares_ref, *refs):
    out_ref = refs[-1]
    n_sub = total_ref.shape[0] // 2
    for half in range(2):
        piece = refs[half]
        squares = squares_ref[half * SPARE : (half + 1) * SPARE, :] + piece[n_sub:, :].astype(F32)
        squares = jnp.sum(squares, axis=0, keepdims=True)
        scale = lax.rsqrt(squares / features + EPSILON)
        scale = jnp.broadcast_to(scale, (128, scale.shape[1])).T
        for low, high, which in spans[half]:
            rows = slice(half * n_sub + low, half * n_sub + high)
            total = total_ref[rows, :] + times(piece[low:high, :], (w_ref, sw_ref)[which][...])
            n = total.shape[1] // 2
            gate, up = total[:, :n] * scale[low:high, :n], total[:, n:] * scale[low:high, :n]
            hidden = (gate / (1.0 + jnp.exp(-gate)) * up).astype(BF)
            for j in range(out_ref.shape[0]):
                out_ref[j, rows, :] = hidden


def down_kernel(at_ref, hidden_ref, own_ref, got_ref, out_ref):
    core = at_ref[0]
    feat = own_ref.shape[2]
    slots = out_ref.shape[0]
    hidden = jnp.concatenate([hidden_ref[j, :slots, :] for j in range(hidden_ref.shape[0])], axis=1)
    for w, where in ((own_ref.at[core], core), (got_ref, 1 - core)):
        at = pl.ds(pl.multiple_of(where * feat, feat), feat)
        out_ref[:, at] = jnp.dot(
            hidden, w[: hidden.shape[1], :], preferred_element_type=F32
        ).astype(BF)


def pack_kernel(at_ref, *refs):
    arrays, out_ref = refs[:-1], refs[-1]
    rows = out_ref.shape[0] // len(arrays)
    for i, a in enumerate(arrays):
        part = a.at[1 - at_ref[0]] if len(a.shape) == 3 else a
        out_ref[i * rows : (i + 1) * rows, :] = part[...]


def call(kernel, out, args, flops, mib, scratch=()):
    return pl.pallas_call(
        kernel,
        out_shape=out,
        in_specs=[SMEM] + [VMEM] * (len(args) - 1),
        out_specs=jax.tree.map(lambda _: VMEM, out),
        scratch_shapes=scratch,
        cost_estimate=pl.CostEstimate(flops=flops, bytes_accessed=2**21, transcendentals=0),
        compiler_params=pltpu.CompilerParams(vmem_limit_bytes=mib * 2**20),
    )(*args)


def body(
    tokens,
    pre_gain,
    expert_ids,
    route_weight,
    expert_gate,
    expert_up,
    expert_down,
    shared_gate,
    shared_up,
    shared_down,
    out_gain,
):
    tok, top = expert_ids.shape
    n_ep = lax.axis_size("ep")
    n_tp = lax.axis_size("tp")
    n_y = n_tp // 2
    experts = expert_gate.shape[0] * n_ep
    cap = 4 * tok * top // (3 * experts)
    feat = tokens.shape[1]
    feat_all = feat * n_tp
    width = 2 * feat
    hid = expert_gate.shape[1]
    n_hid = expert_down.shape[1]
    half = tok // 2
    slots = n_ep * cap
    rows = slots + half
    n_sub = rows // 2
    tp = lax.axis_index("tp")
    core = lax.rem(tp, 2)
    y = lax.div(tp, 2)
    first = core == 0
    place = jnp.stack([core, y]).astype(jnp.int32)

    swap = [(i, i ^ 1) for i in range(n_tp)]
    y_groups = [[c + 2 * k for k in range(n_y)] for c in range(2)]

    def y_shift(d):
        return [(i, ((i // 2 + d) % n_y) * 2 + i % 2) for i in range(n_tp)]

    def own_first(mine, other, axis):
        return jnp.where(
            first,
            jnp.concatenate([mine, other], axis=axis),
            jnp.concatenate([other, mine], axis=axis),
        )

    partner = lax.ppermute(tokens, "tp", swap)
    ids = expert_ids.T
    outgoing = call(
        functools.partial(route_kernel, n_ep, cap),
        jax.ShapeDtypeStruct((slots, width), BF),
        (place, ids, tokens, partner),
        10**8,
        60,
    )
    arrived = lax.all_to_all(outgoing.reshape(n_ep, cap, width), "ep", 0, 0, tiled=True)
    arrived = arrived.reshape(slots, width)

    gain = own_first(pre_gain, lax.ppermute(pre_gain, "tp", swap), 0)[None, :]
    sent_in = call(
        pack_kernel,
        jax.ShapeDtypeStruct((4 * hid, feat_all), BF),
        (place, expert_gate, expert_up, shared_gate, shared_up),
        4 * 10**8,
        8,
    )
    got_in = lax.ppermute(sent_in, "tp", swap)
    sent_out = call(
        pack_kernel,
        jax.ShapeDtypeStruct((2 * n_hid, feat), BF),
        (place, expert_down, shared_down),
        4 * 10**8,
        6,
    )
    got_out = lax.ppermute(sent_out, "tp", swap)

    piece = jax.ShapeDtypeStruct((n_sub + SPARE, width), BF)
    fwd = call(arrive_kernel, (piece, piece), (place, arrived, tokens, partner, gain), 4 * 10**8, 8)
    fwd, bwd = list(fwd), list(fwd)
    spans = (((0, n_sub, 0),), ((0, slots - n_sub, 0), (slots - n_sub, n_sub, 1)))
    early, early_at = list(fwd), [(0, 0), (1, 0)]
    late, late_at = [], []
    for step in range(1, n_y // 2 + 1):
        last = step == n_y // 2
        pieces, at = (late, late_at) if last else (early, early_at)
        for k in range(2):
            if not last or k == 0:
                fwd[k] = lax.ppermute(fwd[k], "tp", y_shift(1))
                pieces.append(fwd[k])
                at.append((k, -step))
            if not last or k == 1:
                bwd[k] = lax.ppermute(bwd[k], "tp", y_shift(-1))
                pieces.append(bwd[k])
                at.append((k, step))

    flops = 2 * rows * feat_all * 4 * hid
    total, squares, w_last, sw_last = call(
        functools.partial(early_kernel, early_at, spans, n_y, width),
        (
            jax.ShapeDtypeStruct((rows, 4 * hid), F32),
            jax.ShapeDtypeStruct((2 * SPARE, width), F32),
            jax.ShapeDtypeStruct((4 * hid, width), BF),
            jax.ShapeDtypeStruct((4 * hid, width), BF),
        ),
        (place, expert_gate, expert_up, shared_gate, shared_up, got_in, *early),
        flops,
        20,
        [pltpu.VMEM((4 * hid, feat_all), BF), pltpu.VMEM((4 * hid, feat_all), BF)],
    )
    hidden = call(
        lambda _, *refs: late_kernel(spans, feat_all, *refs),
        jax.ShapeDtypeStruct((n_y, rows, 2 * hid), BF),
        (place, w_last, sw_last, total, squares, *late),
        flops // 8,
        8,
    )

    hidden_all = lax.all_to_all(hidden, "tp", 0, 0, axis_index_groups=y_groups, tiled=True)
    expert_out = call(
        down_kernel,
        jax.ShapeDtypeStruct((slots, width), BF),
        (place, hidden_all, expert_down, got_out),
        2 * slots * n_hid * width,
        12,
    )
    returned = lax.all_to_all(expert_out.reshape(n_ep, cap, width), "ep", 0, 0, tiled=True)
    returned = returned.reshape(slots, width)

    sdown_w = own_first(shared_down, got_out[n_hid:], 1).reshape(n_y, 2 * hid, width)
    contract = (((0, 2), (0, 1)), ((), ()))
    shared_out = lax.dot_general(hidden_all[:, slots:], sdown_w, contract, preferred_element_type=F32)
    third = jax.ShapeDtypeStruct((tok, slots), BF)
    mix = call(
        functools.partial(mix_kernel, n_ep, cap),
        (third, third, third),
        (place, ids, route_weight.T),
        4 * 10**8,
        8,
    )
    value = jax.ShapeDtypeStruct((tok, feat), F32)
    home, away = call(
        combine_kernel, (value, value), (place, *mix, returned, shared_out), 6 * tok * slots * width, 8
    )
    summed = home + lax.ppermute(away, "tp", swap)
    own_square = jnp.sum(summed * summed, axis=1)
    sent = jnp.broadcast_to(own_square[None, :], (n_tp, tok))
    out_square = jnp.sum(lax.all_to_all(sent, "tp", 0, 0, tiled=True), axis=0)
    return (summed * lax.rsqrt(out_square[:, None] / feat_all + EPSILON) * out_gain).astype(BF)


def solution(mesh):
    return jax.shard_map(
        body,
        mesh=mesh,
        in_specs=(
            P("ep", "tp"),
            P("tp"),
            P("ep", None),
            P("ep", None),
            P("ep", "tp", None),
            P("ep", "tp", None),
            P("ep", None, "tp"),
            P("tp", None),
            P("tp", None),
            P(None, "tp"),
            P("tp"),
        ),
        out_specs=P("ep", "tp"),
        check_vma=False,
    )
```

```python
import functools

import jax
import jax.numpy as jnp
from jax import lax
from jax.experimental import pallas as pl
from jax.experimental.pallas import tpu as pltpu
from jax.sharding import PartitionSpec as P


EPSILON = 1e-06
BF = jnp.bfloat16
F32 = jnp.float32
SPARE = 8


VMEM = pl.BlockSpec(memory_space=pltpu.VMEM)


def times(x, w):
    return lax.dot_general(x, w, (((1,), (1,)), ((), ())), preferred_element_type=F32)


def here():
    tp = lax.axis_index("tp")
    return lax.rem(tp, 2), lax.div(tp, 2)


def thirds(v):
    high = v.astype(BF)
    rest = v - high.astype(F32)
    middle = rest.astype(BF)
    return high, middle, (rest - middle.astype(F32)).astype(BF)


def picks(ids, core, n_ep, cap, weight=None):
    tok = ids.shape[1]
    named = 2 * lax.broadcasted_iota(jnp.int32, (n_ep, tok), 0) + core
    member = ids[0:1, :] == named
    for k in range(1, ids.shape[0]):
        member = member | (ids[k : k + 1, :] == named)
    before = lax.broadcasted_iota(jnp.int32, (tok, tok), 0) < lax.broadcasted_iota(jnp.int32, (tok, tok), 1)
    one = jnp.where(member, 1.0, 0.0).astype(BF)
    rank = jnp.dot(one, jnp.where(before, 1.0, 0.0).astype(BF), preferred_element_type=F32)
    rank = jnp.where(member, rank, -1.0)
    spread = jnp.broadcast_to(rank[:, None, :], (n_ep, cap, tok))
    slot = lax.broadcasted_iota(jnp.int32, (n_ep, cap, tok), 1).astype(F32)
    if weight is None:
        return jnp.where(spread == slot, 1.0, 0.0).astype(BF).reshape(n_ep * cap, tok)
    value = jnp.where(ids[0:1, :] == named, weight[0:1, :], 0.0)
    for k in range(1, ids.shape[0]):
        value = value + jnp.where(ids[k : k + 1, :] == named, weight[k : k + 1, :], 0.0)
    value = jnp.broadcast_to(value[:, None, :], (n_ep, cap, tok))
    return jnp.where(spread == slot, value, 0.0).reshape(n_ep * cap, tok)


def mix_kernel(n_ep, cap, ids_ref, weight_ref, *out_refs):
    mix = picks(ids_ref[...], here()[0], n_ep, cap, weight_ref[...]).T
    for ref, value in zip(out_refs, thirds(mix)):
        ref[...] = value


def combine_kernel(high, middle, low, rows_ref, shared_ref, home_ref, away_ref):
    core, _ = here()
    rows = rows_ref[...]
    part = jnp.dot(high[...], rows, preferred_element_type=F32)
    part = part + jnp.dot(middle[...], rows, preferred_element_type=F32)
    part = part + jnp.dot(low[...], rows, preferred_element_type=F32)
    shared = shared_ref[...]
    half, feat = shared.shape[0], home_ref.shape[1]
    top = part[:half] + jnp.where(core == 0, shared, 0.0)
    bottom = part[half:] + jnp.where(core == 0, 0.0, shared)
    for at, value in ((slice(0, half), top), (slice(half, 2 * half), bottom)):
        left, right = value[:, :feat], value[:, feat:]
        home_ref[at, :] = jnp.where(core == 0, left, right)
        away_ref[at, :] = jnp.where(core == 0, right, left)


def route_kernel(n_ep, cap, ids_ref, own_ref, other_ref, out_ref):
    core, _ = here()
    one_hot = picks(ids_ref[...], core, n_ep, cap)
    feat = own_ref.shape[1]
    for ref, where in ((own_ref, core), (other_ref, 1 - core)):
        at = pl.ds(pl.multiple_of(where * feat, feat), feat)
        out_ref[:, at] = jnp.dot(one_hot, ref[...], preferred_element_type=F32).astype(BF)


def arrive_kernel(rows_ref, own_ref, other_ref, gain_ref, first_ref, second_ref):
    core, _ = here()
    slots, width = rows_ref.shape
    half, feat = own_ref.shape[0] // 2, own_ref.shape[1]
    n_sub = (slots + half) // 2
    mine = pl.ds(pl.multiple_of(core * half, half), half)
    own, other = own_ref[mine, :], other_ref[mine, :]
    own, other = jnp.where(core == 0, own, other), jnp.where(core == 0, other, own)
    split = slots - n_sub
    gain = gain_ref[...]

    def put(ref, at, rows, columns):
        raw = rows.astype(F32)
        ref[at : at + rows.shape[0], columns] = (raw * gain[:, columns]).astype(BF)
        return raw * raw

    every, left, right = slice(0, width), slice(0, feat), slice(feat, width)

    def total(squares):
        ones = jnp.ones((SPARE, squares.shape[1]), F32)
        return lax.dot_general(
            ones, squares, (((1,), (1,)), ((), ())), precision=lax.Precision.HIGHEST, preferred_element_type=F32
        )

    def spare(ref, at, sums):
        high, middle, low = thirds(sums)
        row = lax.broadcasted_iota(jnp.int32, sums.shape, 0)
        parts = jnp.where(row == 0, high.astype(F32), jnp.where(row == 1, middle.astype(F32), low.astype(F32)))
        ref[n_sub:, at : at + sums.shape[1]] = jnp.where(row < 3, parts, 0.0).astype(BF)

    for ref in (first_ref, second_ref):
        ref[n_sub:, :] = jnp.zeros((SPARE, width), BF)
    spare(first_ref, 0, total(put(first_ref, 0, rows_ref[:n_sub, :], every)))
    sums = total(put(second_ref, 0, rows_ref[n_sub:, :], every))
    tail = total(put(second_ref, split, own, left)) + total(put(second_ref, split, other, right))
    spare(second_ref, 0, jnp.concatenate([sums, tail], axis=1))


def early_kernel(places, spans, n_y, width, gate, up, s_gate, s_up, got, *refs):
    n = len(places)
    pieces = refs[:n]
    total_ref, squares_ref, w_last, sw_last, w, sw = refs[n:]
    core, y = here()
    hid = s_gate.shape[0]
    n_sub = total_ref.shape[0] // 2
    own = pl.multiple_of(core * hid, hid)
    other = pl.multiple_of((1 - core) * hid, hid)
    for i, (mine, into, base) in enumerate(
        ((gate.at[core], w, 0), (up.at[core], w, 2 * hid), (s_gate, sw, 0), (s_up, sw, 2 * hid))
    ):
        into[pl.ds(base + own, hid), :] = mine[...]
        into[pl.ds(base + other, hid), :] = got[i * hid : (i + 1) * hid, :]

    def columns(offset):
        return pl.ds(pl.multiple_of(lax.rem(y + offset * (1 - 2 * core) + n_y, n_y) * width, width), width)

    for half in range(2):
        total = [None] * len(spans[half])
        squares = jnp.zeros((SPARE, width), F32)
        for piece, (k, offset) in zip(pieces, places):
            if k != half:
                continue
            for j, (low, high, which) in enumerate(spans[half]):
                term = times(piece[low:high, :], (w, sw)[which][:, columns(offset)])
                total[j] = term if total[j] is None else total[j] + term
            squares = squares + piece[n_sub:, :].astype(F32)
        for (low, high, _), value in zip(spans[half], total):
            total_ref[half * n_sub + low : half * n_sub + high, :] = value
        squares_ref[half * SPARE : (half + 1) * SPARE, :] = squares
    w_last[...] = w[:, columns(n_y // 2)]
    sw_last[...] = sw[:, columns(n_y // 2)]


def late_kernel(spans, features, w_ref, sw_ref, total_ref, squares_ref, *refs):
    out_ref = refs[-1]
    n_sub = total_ref.shape[0] // 2
    for half in range(2):
        piece = refs[half]
        squares = squares_ref[half * SPARE : (half + 1) * SPARE, :] + piece[n_sub:, :].astype(F32)
        squares = jnp.sum(squares, axis=0, keepdims=True)
        scale = lax.rsqrt(squares / features + EPSILON)
        scale = jnp.broadcast_to(scale, (128, scale.shape[1])).T
        for low, high, which in spans[half]:
            rows = slice(half * n_sub + low, half * n_sub + high)
            total = total_ref[rows, :] + times(piece[low:high, :], (w_ref, sw_ref)[which][...])
            n = total.shape[1] // 2
            gate, up = total[:, :n] * scale[low:high, :n], total[:, n:] * scale[low:high, :n]
            hidden = (gate / (1.0 + jnp.exp(-gate)) * up).astype(BF)
            for j in range(out_ref.shape[0]):
                out_ref[j, rows, :] = hidden


def down_kernel(hidden_ref, own_ref, got_ref, out_ref):
    core, _ = here()
    feat = own_ref.shape[2]
    slots = out_ref.shape[0]
    hidden = jnp.concatenate([hidden_ref[j, :slots, :] for j in range(hidden_ref.shape[0])], axis=1)
    for w, where in ((own_ref.at[core], core), (got_ref, 1 - core)):
        at = pl.ds(pl.multiple_of(where * feat, feat), feat)
        out_ref[:, at] = jnp.dot(
            hidden, w[: hidden.shape[1], :], preferred_element_type=F32
        ).astype(BF)


def pack_kernel(*refs):
    arrays, out_ref = refs[:-1], refs[-1]
    rows = out_ref.shape[0] // len(arrays)
    for i, a in enumerate(arrays):
        part = a.at[1 - here()[0]] if len(a.shape) == 3 else a
        out_ref[i * rows : (i + 1) * rows, :] = part[...]


def call(kernel, out, args, flops, mib, scratch=()):
    return pl.pallas_call(
        kernel,
        out_shape=out,
        in_specs=[VMEM] * len(args),
        out_specs=jax.tree.map(lambda _: VMEM, out),
        scratch_shapes=scratch,
        cost_estimate=pl.CostEstimate(flops=flops, bytes_accessed=2**21, transcendentals=0),
        compiler_params=pltpu.CompilerParams(vmem_limit_bytes=mib * 2**20),
    )(*args)


def body(
    tokens,
    pre_gain,
    expert_ids,
    route_weight,
    expert_gate,
    expert_up,
    expert_down,
    shared_gate,
    shared_up,
    shared_down,
    out_gain,
):
    tok, top = expert_ids.shape
    n_ep = lax.axis_size("ep")
    n_tp = lax.axis_size("tp")
    n_y = n_tp // 2
    experts = expert_gate.shape[0] * n_ep
    cap = 4 * tok * top // (3 * experts)
    feat = tokens.shape[1]
    feat_all = feat * n_tp
    width = 2 * feat
    hid = expert_gate.shape[1]
    n_hid = expert_down.shape[1]
    half = tok // 2
    slots = n_ep * cap
    rows = slots + half
    n_sub = rows // 2
    tp = lax.axis_index("tp")
    core = lax.rem(tp, 2)
    y = lax.div(tp, 2)
    first = core == 0

    swap = [(i, i ^ 1) for i in range(n_tp)]
    y_groups = [[c + 2 * k for k in range(n_y)] for c in range(2)]

    def y_shift(d):
        return [(i, ((i // 2 + d * (1 - 2 * (i % 2))) % n_y) * 2 + i % 2) for i in range(n_tp)]

    def own_first(mine, other, axis):
        return jnp.where(
            first,
            jnp.concatenate([mine, other], axis=axis),
            jnp.concatenate([other, mine], axis=axis),
        )

    partner = lax.ppermute(tokens, "tp", swap)
    ids = expert_ids.T
    outgoing = call(
        functools.partial(route_kernel, n_ep, cap),
        jax.ShapeDtypeStruct((slots, width), BF),
        (ids, tokens, partner),
        10**8,
        60,
    )
    arrived = lax.all_to_all(outgoing.reshape(n_ep, cap, width), "ep", 0, 0, tiled=True)
    arrived = arrived.reshape(slots, width)

    gain = own_first(pre_gain, lax.ppermute(pre_gain, "tp", swap), 0)[None, :]
    sent_in = call(
        pack_kernel,
        jax.ShapeDtypeStruct((4 * hid, feat_all), BF),
        (expert_gate, expert_up, shared_gate, shared_up),
        4 * 10**8,
        8,
    )
    got_in = lax.ppermute(sent_in, "tp", swap)
    sent_out = call(
        pack_kernel,
        jax.ShapeDtypeStruct((2 * n_hid, feat), BF),
        (expert_down, shared_down),
        4 * 10**8,
        6,
    )
    got_out = lax.ppermute(sent_out, "tp", swap)

    piece = jax.ShapeDtypeStruct((n_sub + SPARE, width), BF)
    fwd = call(
        arrive_kernel, (piece, piece), (arrived, tokens, partner, gain), 4 * 10**8, 8
    )
    fwd, bwd = list(fwd), list(fwd)
    spans = (((0, n_sub, 0),), ((0, slots - n_sub, 0), (slots - n_sub, n_sub, 1)))
    early, early_at = list(fwd), [(0, 0), (1, 0)]
    late, late_at = [], []
    for step in range(1, n_y // 2 + 1):
        last = step == n_y // 2
        pieces, at = (late, late_at) if last else (early, early_at)
        for k in range(2):
            if not last or k == 0:
                fwd[k] = lax.ppermute(fwd[k], "tp", y_shift(1))
                pieces.append(fwd[k])
                at.append((k, -step))
            if not last or k == 1:
                bwd[k] = lax.ppermute(bwd[k], "tp", y_shift(-1))
                pieces.append(bwd[k])
                at.append((k, step))

    flops = 2 * rows * feat_all * 4 * hid
    total, squares, w_last, sw_last = call(
        functools.partial(early_kernel, early_at, spans, n_y, width),
        (
            jax.ShapeDtypeStruct((rows, 4 * hid), F32),
            jax.ShapeDtypeStruct((2 * SPARE, width), F32),
            jax.ShapeDtypeStruct((4 * hid, width), BF),
            jax.ShapeDtypeStruct((4 * hid, width), BF),
        ),
        (expert_gate, expert_up, shared_gate, shared_up, got_in, *early),
        flops,
        20,
        [pltpu.VMEM((4 * hid, feat_all), BF), pltpu.VMEM((4 * hid, feat_all), BF)],
    )
    hidden = call(
        functools.partial(late_kernel, spans, feat_all),
        jax.ShapeDtypeStruct((n_y, rows, 2 * hid), BF),
        (w_last, sw_last, total, squares, *late),
        flops // 8,
        8,
    )

    hidden_all = lax.all_to_all(hidden, "tp", 0, 0, axis_index_groups=y_groups, tiled=True)
    expert_out = call(
        down_kernel,
        jax.ShapeDtypeStruct((slots, width), BF),
        (hidden_all, expert_down, got_out),
        2 * slots * n_hid * width,
        12,
    )
    returned = lax.all_to_all(expert_out.reshape(n_ep, cap, width), "ep", 0, 0, tiled=True)
    returned = returned.reshape(slots, width)

    sdown_w = own_first(shared_down, got_out[n_hid:], 1).reshape(n_y, 2 * hid, width)
    contract = (((0, 2), (0, 1)), ((), ()))
    shared_out = lax.dot_general(hidden_all[:, slots:], sdown_w, contract, preferred_element_type=F32)
    third = jax.ShapeDtypeStruct((tok, slots), BF)
    mix = call(
        functools.partial(mix_kernel, n_ep, cap),
        (third, third, third),
        (ids, route_weight.T),
        4 * 10**8,
        8,
    )
    value = jax.ShapeDtypeStruct((tok, feat), F32)
    home, away = call(
        combine_kernel, (value, value), (*mix, returned, shared_out), 6 * tok * slots * width, 8
    )
    summed = home + lax.ppermute(away, "tp", swap)
    own_square = jnp.sum(summed * summed, axis=1)
    sent = jnp.broadcast_to(own_square[None, :], (n_tp, tok))
    out_square = jnp.sum(lax.all_to_all(sent, "tp", 0, 0, tiled=True), axis=0)
    return (summed * lax.rsqrt(out_square[:, None] / feat_all + EPSILON) * out_gain).astype(BF)


def solution(mesh):
    return jax.shard_map(
        body,
        mesh=mesh,
        in_specs=(
            P("ep", "tp"),
            P("tp"),
            P("ep", None),
            P("ep", None),
            P("ep", "tp", None),
            P("ep", "tp", None),
            P("ep", None, "tp"),
            P("tp", None),
            P("tp", None),
            P(None, "tp"),
            P("tp"),
        ),
        out_specs=P("ep", "tp"),
        check_vma=False,
    )
```

```python
import functools

import jax
import jax.numpy as jnp
from jax import lax
from jax.experimental import pallas as pl
from jax.experimental.pallas import tpu as pltpu
from jax.sharding import PartitionSpec as P


EPSILON = 1e-06
BF = jnp.bfloat16
F32 = jnp.float32
SPARE = 8


VMEM = pl.BlockSpec(memory_space=pltpu.VMEM)


def times(x, w):
    return lax.dot_general(x, w, (((1,), (1,)), ((), ())), preferred_element_type=F32)


def here():
    tp = lax.axis_index("tp")
    return lax.rem(tp, 2), lax.div(tp, 2)


def thirds(v):
    high = v.astype(BF)
    rest = v - high.astype(F32)
    middle = rest.astype(BF)
    return high, middle, (rest - middle.astype(F32)).astype(BF)


def picks(ids, core, n_ep, cap, weight=None):
    tok = ids.shape[1]
    named = 2 * lax.broadcasted_iota(jnp.int32, (n_ep, tok), 0) + core
    member = ids[0:1, :] == named
    for k in range(1, ids.shape[0]):
        member = member | (ids[k : k + 1, :] == named)
    before = lax.broadcasted_iota(jnp.int32, (tok, tok), 0) < lax.broadcasted_iota(jnp.int32, (tok, tok), 1)
    one = jnp.where(member, 1.0, 0.0).astype(BF)
    rank = jnp.dot(one, jnp.where(before, 1.0, 0.0).astype(BF), preferred_element_type=F32)
    rank = jnp.where(member, rank, -1.0)
    spread = jnp.broadcast_to(rank[:, None, :], (n_ep, cap, tok))
    slot = lax.broadcasted_iota(jnp.int32, (n_ep, cap, tok), 1).astype(F32)
    if weight is None:
        return jnp.where(spread == slot, 1.0, 0.0).astype(BF).reshape(n_ep * cap, tok)
    value = jnp.where(ids[0:1, :] == named, weight[0:1, :], 0.0)
    for k in range(1, ids.shape[0]):
        value = value + jnp.where(ids[k : k + 1, :] == named, weight[k : k + 1, :], 0.0)
    value = jnp.broadcast_to(value[:, None, :], (n_ep, cap, tok))
    return jnp.where(spread == slot, value, 0.0).reshape(n_ep * cap, tok)


def mix_kernel(n_ep, cap, ids_ref, weight_ref, *out_refs):
    mix = picks(ids_ref[...], here()[0], n_ep, cap, weight_ref[...]).T
    for ref, value in zip(out_refs, thirds(mix)):
        ref[...] = value


def combine_kernel(high, middle, low, rows_ref, shared_ref, home_ref, away_ref):
    core, _ = here()
    rows = rows_ref[...]
    part = jnp.dot(high[...], rows, preferred_element_type=F32)
    part = part + jnp.dot(middle[...], rows, preferred_element_type=F32)
    part = part + jnp.dot(low[...], rows, preferred_element_type=F32)
    shared = shared_ref[...]
    half, feat = shared.shape[0], home_ref.shape[1]
    top = part[:half] + jnp.where(core == 0, shared, 0.0)
    bottom = part[half:] + jnp.where(core == 0, 0.0, shared)
    for at, value in ((slice(0, half), top), (slice(half, 2 * half), bottom)):
        left, right = value[:, :feat], value[:, feat:]
        home_ref[at, :] = jnp.where(core == 0, left, right)
        away_ref[at, :] = jnp.where(core == 0, right, left)


def route_kernel(n_ep, cap, ids_ref, own_ref, other_ref, out_ref):
    core, _ = here()
    one_hot = picks(ids_ref[...], core, n_ep, cap)
    feat = own_ref.shape[1]
    for ref, where in ((own_ref, core), (other_ref, 1 - core)):
        at = pl.ds(pl.multiple_of(where * feat, feat), feat)
        out_ref[:, at] = jnp.dot(one_hot, ref[...], preferred_element_type=F32).astype(BF)


def arrive_kernel(rows_ref, own_ref, other_ref, gain_ref, first_ref, second_ref):
    core, _ = here()
    slots, width = rows_ref.shape
    half, feat = own_ref.shape[0] // 2, own_ref.shape[1]
    n_sub = (slots + half) // 2
    mine = pl.ds(pl.multiple_of(core * half, half), half)
    own, other = own_ref[mine, :], other_ref[mine, :]
    own, other = jnp.where(core == 0, own, other), jnp.where(core == 0, other, own)
    split = slots - n_sub
    gain = gain_ref[...]

    def put(ref, at, rows, columns):
        raw = rows.astype(F32)
        ref[at : at + rows.shape[0], columns] = (raw * gain[:, columns]).astype(BF)
        return raw * raw

    every, left, right = slice(0, width), slice(0, feat), slice(feat, width)

    def total(squares):
        ones = jnp.ones((SPARE, squares.shape[1]), BF)
        high, middle, low = (times(ones, part) for part in thirds(squares))
        return high + middle + low

    def spare(ref, at, sums):
        high, middle, low = thirds(sums)
        row = lax.broadcasted_iota(jnp.int32, sums.shape, 0)
        parts = jnp.where(row == 0, high.astype(F32), jnp.where(row == 1, middle.astype(F32), low.astype(F32)))
        ref[n_sub:, at : at + sums.shape[1]] = jnp.where(row < 3, parts, 0.0).astype(BF)

    for ref in (first_ref, second_ref):
        ref[n_sub:, :] = jnp.zeros((SPARE, width), BF)
    spare(first_ref, 0, total(put(first_ref, 0, rows_ref[:n_sub, :], every)))
    sums = total(put(second_ref, 0, rows_ref[n_sub:, :], every))
    tail = total(put(second_ref, split, own, left)) + total(put(second_ref, split, other, right))
    spare(second_ref, 0, jnp.concatenate([sums, tail], axis=1))


def early_kernel(places, spans, n_y, width, gate, up, s_gate, s_up, got, *refs):
    n = len(places)
    pieces = refs[:n]
    total_ref, squares_ref, w_last, sw_last, w, sw = refs[n:]
    core, y = here()
    hid = s_gate.shape[0]
    n_sub = total_ref.shape[0] // 2
    own = pl.multiple_of(core * hid, hid)
    other = pl.multiple_of((1 - core) * hid, hid)
    for i, (mine, into, base) in enumerate(
        ((gate.at[core], w, 0), (up.at[core], w, 2 * hid), (s_gate, sw, 0), (s_up, sw, 2 * hid))
    ):
        into[pl.ds(base + own, hid), :] = mine[...]
        into[pl.ds(base + other, hid), :] = got[i * hid : (i + 1) * hid, :]

    def columns(offset):
        return pl.ds(pl.multiple_of(lax.rem(y + offset + n_y, n_y) * width, width), width)

    for half in range(2):
        total = [None] * len(spans[half])
        squares = jnp.zeros((SPARE, width), F32)
        for piece, (k, offset) in zip(pieces, places):
            if k != half:
                continue
            for j, (low, high, which) in enumerate(spans[half]):
                term = times(piece[low:high, :], (w, sw)[which][:, columns(offset)])
                total[j] = term if total[j] is None else total[j] + term
            squares = squares + piece[n_sub:, :].astype(F32)
        for (low, high, _), value in zip(spans[half], total):
            total_ref[half * n_sub + low : half * n_sub + high, :] = value
        squares_ref[half * SPARE : (half + 1) * SPARE, :] = squares
    w_last[...] = w[:, columns(n_y // 2)]
    sw_last[...] = sw[:, columns(n_y // 2)]


def late_kernel(spans, features, w_ref, sw_ref, total_ref, squares_ref, *refs):
    out_ref = refs[-1]
    n_sub = total_ref.shape[0] // 2
    for half in range(2):
        piece = refs[half]
        squares = squares_ref[half * SPARE : (half + 1) * SPARE, :] + piece[n_sub:, :].astype(F32)
        squares = jnp.sum(squares, axis=0, keepdims=True)
        scale = lax.rsqrt(squares / features + EPSILON)
        scale = jnp.broadcast_to(scale, (128, scale.shape[1])).T
        for low, high, which in spans[half]:
            rows = slice(half * n_sub + low, half * n_sub + high)
            total = total_ref[rows, :] + times(piece[low:high, :], (w_ref, sw_ref)[which][...])
            n = total.shape[1] // 2
            gate, up = total[:, :n] * scale[low:high, :n], total[:, n:] * scale[low:high, :n]
            hidden = (gate / (1.0 + jnp.exp(-gate)) * up).astype(BF)
            for j in range(out_ref.shape[0]):
                out_ref[j, rows, :] = hidden


def down_kernel(hidden_ref, own_ref, got_ref, out_ref):
    core, _ = here()
    feat = own_ref.shape[2]
    slots = out_ref.shape[0]
    hidden = jnp.concatenate([hidden_ref[j, :slots, :] for j in range(hidden_ref.shape[0])], axis=1)
    for w, where in ((own_ref.at[core], core), (got_ref, 1 - core)):
        at = pl.ds(pl.multiple_of(where * feat, feat), feat)
        out_ref[:, at] = jnp.dot(
            hidden, w[: hidden.shape[1], :], preferred_element_type=F32
        ).astype(BF)


def pack_kernel(*refs):
    arrays, out_ref = refs[:-1], refs[-1]
    rows = out_ref.shape[0] // len(arrays)
    for i, a in enumerate(arrays):
        part = a.at[1 - here()[0]] if len(a.shape) == 3 else a
        out_ref[i * rows : (i + 1) * rows, :] = part[...]


def call(kernel, out, args, flops, mib, scratch=()):
    return pl.pallas_call(
        kernel,
        out_shape=out,
        in_specs=[VMEM] * len(args),
        out_specs=jax.tree.map(lambda _: VMEM, out),
        scratch_shapes=scratch,
        cost_estimate=pl.CostEstimate(flops=flops, bytes_accessed=2**21, transcendentals=0),
        compiler_params=pltpu.CompilerParams(vmem_limit_bytes=mib * 2**20),
    )(*args)


def body(
    tokens,
    pre_gain,
    expert_ids,
    route_weight,
    expert_gate,
    expert_up,
    expert_down,
    shared_gate,
    shared_up,
    shared_down,
    out_gain,
):
    tok, top = expert_ids.shape
    n_ep = lax.axis_size("ep")
    n_tp = lax.axis_size("tp")
    n_y = n_tp // 2
    experts = expert_gate.shape[0] * n_ep
    cap = 4 * tok * top // (3 * experts)
    feat = tokens.shape[1]
    feat_all = feat * n_tp
    width = 2 * feat
    hid = expert_gate.shape[1]
    n_hid = expert_down.shape[1]
    half = tok // 2
    slots = n_ep * cap
    rows = slots + half
    n_sub = rows // 2
    tp = lax.axis_index("tp")
    core = lax.rem(tp, 2)
    y = lax.div(tp, 2)
    first = core == 0

    swap = [(i, i ^ 1) for i in range(n_tp)]
    y_groups = [[c + 2 * k for k in range(n_y)] for c in range(2)]

    def y_shift(d):
        return [(i, ((i // 2 + d) % n_y) * 2 + i % 2) for i in range(n_tp)]

    def own_first(mine, other, axis):
        return jnp.where(
            first,
            jnp.concatenate([mine, other], axis=axis),
            jnp.concatenate([other, mine], axis=axis),
        )

    partner = lax.ppermute(tokens, "tp", swap)
    ids = expert_ids.T
    outgoing = call(
        functools.partial(route_kernel, n_ep, cap),
        jax.ShapeDtypeStruct((slots, width), BF),
        (ids, tokens, partner),
        10**8,
        60,
    )
    arrived = lax.all_to_all(outgoing.reshape(n_ep, cap, width), "ep", 0, 0, tiled=True)
    arrived = arrived.reshape(slots, width)

    gain = own_first(pre_gain, lax.ppermute(pre_gain, "tp", swap), 0)[None, :]
    sent_in = call(
        pack_kernel,
        jax.ShapeDtypeStruct((4 * hid, feat_all), BF),
        (expert_gate, expert_up, shared_gate, shared_up),
        4 * 10**8,
        8,
    )
    got_in = lax.ppermute(sent_in, "tp", swap)
    sent_out = call(
        pack_kernel,
        jax.ShapeDtypeStruct((2 * n_hid, feat), BF),
        (expert_down, shared_down),
        4 * 10**8,
        6,
    )
    got_out = lax.ppermute(sent_out, "tp", swap)

    piece = jax.ShapeDtypeStruct((n_sub + SPARE, width), BF)
    fwd = call(
        arrive_kernel, (piece, piece), (arrived, tokens, partner, gain), 4 * 10**8, 8
    )
    fwd, bwd = list(fwd), list(fwd)
    spans = (((0, n_sub, 0),), ((0, slots - n_sub, 0), (slots - n_sub, n_sub, 1)))
    early, early_at = list(fwd), [(0, 0), (1, 0)]
    late, late_at = [], []
    for step in range(1, n_y // 2 + 1):
        last = step == n_y // 2
        pieces, at = (late, late_at) if last else (early, early_at)
        for k in range(2):
            if not last or k == 0:
                fwd[k] = lax.ppermute(fwd[k], "tp", y_shift(1))
                pieces.append(fwd[k])
                at.append((k, -step))
            if not last or k == 1:
                bwd[k] = lax.ppermute(bwd[k], "tp", y_shift(-1))
                pieces.append(bwd[k])
                at.append((k, step))

    flops = 2 * rows * feat_all * 4 * hid
    total, squares, w_last, sw_last = call(
        functools.partial(early_kernel, early_at, spans, n_y, width),
        (
            jax.ShapeDtypeStruct((rows, 4 * hid), F32),
            jax.ShapeDtypeStruct((2 * SPARE, width), F32),
            jax.ShapeDtypeStruct((4 * hid, width), BF),
            jax.ShapeDtypeStruct((4 * hid, width), BF),
        ),
        (expert_gate, expert_up, shared_gate, shared_up, got_in, *early),
        flops,
        20,
        [pltpu.VMEM((4 * hid, feat_all), BF), pltpu.VMEM((4 * hid, feat_all), BF)],
    )
    hidden = call(
        functools.partial(late_kernel, spans, feat_all),
        jax.ShapeDtypeStruct((n_y, rows, 2 * hid), BF),
        (w_last, sw_last, total, squares, *late),
        flops // 8,
        8,
    )

    hidden_all = lax.all_to_all(hidden, "tp", 0, 0, axis_index_groups=y_groups, tiled=True)
    expert_out = call(
        down_kernel,
        jax.ShapeDtypeStruct((slots, width), BF),
        (hidden_all, expert_down, got_out),
        2 * slots * n_hid * width,
        12,
    )
    returned = lax.all_to_all(expert_out.reshape(n_ep, cap, width), "ep", 0, 0, tiled=True)
    returned = returned.reshape(slots, width)

    sdown_w = own_first(shared_down, got_out[n_hid:], 1).reshape(n_y, 2 * hid, width)
    contract = (((0, 2), (0, 1)), ((), ()))
    shared_out = lax.dot_general(hidden_all[:, slots:], sdown_w, contract, preferred_element_type=F32)
    third = jax.ShapeDtypeStruct((tok, slots), BF)
    mix = call(
        functools.partial(mix_kernel, n_ep, cap),
        (third, third, third),
        (ids, route_weight.T),
        4 * 10**8,
        60,
    )
    value = jax.ShapeDtypeStruct((tok, feat), F32)
    home, away = call(
        combine_kernel, (value, value), (*mix, returned, shared_out), 6 * tok * slots * width, 8
    )
    summed = home + lax.ppermute(away, "tp", swap)
    own_square = jnp.sum(summed * summed, axis=1)
    sent = jnp.broadcast_to(own_square[None, :], (n_tp, tok))
    out_square = jnp.sum(lax.all_to_all(sent, "tp", 0, 0, tiled=True), axis=0)
    return (summed * lax.rsqrt(out_square[:, None] / feat_all + EPSILON) * out_gain).astype(BF)


def solution(mesh):
    return jax.shard_map(
        body,
        mesh=mesh,
        in_specs=(
            P("ep", "tp"),
            P("tp"),
            P("ep", None),
            P("ep", None),
            P("ep", "tp", None),
            P("ep", "tp", None),
            P("ep", None, "tp"),
            P("tp", None),
            P("tp", None),
            P(None, "tp"),
            P("tp"),
        ),
        out_specs=P("ep", "tp"),
        check_vma=False,
    )
```

```python
import functools

import jax
import jax.numpy as jnp
from jax import lax
from jax.experimental import pallas as pl
from jax.experimental.pallas import tpu as pltpu
from jax.sharding import PartitionSpec as P


EPSILON = 1e-06
BF = jnp.bfloat16
F32 = jnp.float32
SPARE = 8


VMEM = pl.BlockSpec(memory_space=pltpu.VMEM)


def times(x, w):
    return lax.dot_general(x, w, (((1,), (1,)), ((), ())), preferred_element_type=F32)


def here():
    tp = lax.axis_index("tp")
    return lax.rem(tp, 2), lax.div(tp, 2)


def thirds(v):
    high = v.astype(BF)
    rest = v - high.astype(F32)
    middle = rest.astype(BF)
    return high, middle, (rest - middle.astype(F32)).astype(BF)


def picks(ids, core, n_ep, cap, weight=None):
    tok = ids.shape[1]
    named = 2 * lax.broadcasted_iota(jnp.int32, (n_ep, tok), 0) + core
    member = ids[0:1, :] == named
    for k in range(1, ids.shape[0]):
        member = member | (ids[k : k + 1, :] == named)
    before = lax.broadcasted_iota(jnp.int32, (tok, tok), 0) < lax.broadcasted_iota(jnp.int32, (tok, tok), 1)
    one = jnp.where(member, 1.0, 0.0).astype(BF)
    rank = jnp.dot(one, jnp.where(before, 1.0, 0.0).astype(BF), preferred_element_type=F32)
    rank = jnp.where(member, rank, -1.0)
    spread = jnp.broadcast_to(rank[:, None, :], (n_ep, cap, tok))
    slot = lax.broadcasted_iota(jnp.int32, (n_ep, cap, tok), 1).astype(F32)
    if weight is None:
        return jnp.where(spread == slot, 1.0, 0.0).astype(BF).reshape(n_ep * cap, tok)
    value = jnp.where(ids[0:1, :] == named, weight[0:1, :], 0.0)
    for k in range(1, ids.shape[0]):
        value = value + jnp.where(ids[k : k + 1, :] == named, weight[k : k + 1, :], 0.0)
    value = jnp.broadcast_to(value[:, None, :], (n_ep, cap, tok))
    return jnp.where(spread == slot, value, 0.0).reshape(n_ep * cap, tok)


def mix_kernel(n_ep, cap, ids_ref, weight_ref, *out_refs):
    mix = picks(ids_ref[...], here()[0], n_ep, cap, weight_ref[...]).T
    for ref, value in zip(out_refs, thirds(mix)):
        ref[...] = value


def combine_kernel(high, middle, low, rows_ref, shared_ref, home_ref, away_ref):
    core, _ = here()
    rows = rows_ref[...]
    part = jnp.dot(high[...], rows, preferred_element_type=F32)
    part = part + jnp.dot(middle[...], rows, preferred_element_type=F32)
    part = part + jnp.dot(low[...], rows, preferred_element_type=F32)
    shared = shared_ref[...]
    half, feat = shared.shape[0], home_ref.shape[1]
    top = part[:half] + jnp.where(core == 0, shared, 0.0)
    bottom = part[half:] + jnp.where(core == 0, 0.0, shared)
    for at, value in ((slice(0, half), top), (slice(half, 2 * half), bottom)):
        left, right = value[:, :feat], value[:, feat:]
        home_ref[at, :] = jnp.where(core == 0, left, right)
        away_ref[at, :] = jnp.where(core == 0, right, left)


def own_kernel(n_ep, cap, ids_ref, own_ref, pick_ref, part_ref):
    one_hot = picks(ids_ref[...], here()[0], n_ep, cap)
    pick_ref[...] = one_hot
    part_ref[...] = jnp.dot(one_hot, own_ref[...], preferred_element_type=F32).astype(BF)


def join_kernel(pick_ref, part_ref, other_ref, out_ref):
    core, _ = here()
    feat = part_ref.shape[1]
    out_ref[:, pl.ds(pl.multiple_of(core * feat, feat), feat)] = part_ref[...]
    other = jnp.dot(pick_ref[...], other_ref[...], preferred_element_type=F32).astype(BF)
    out_ref[:, pl.ds(pl.multiple_of((1 - core) * feat, feat), feat)] = other


def mix_kernel(n_ep, cap, ids_ref, weight_ref, *out_refs):
    mix = picks(ids_ref[...], here()[0], n_ep, cap, weight_ref[...]).T
    for ref, value in zip(out_refs, thirds(mix)):
        ref[...] = value


def combine_kernel(high, middle, low, rows_ref, shared_ref, home_ref, away_ref):
    core, _ = here()
    rows = rows_ref[...]
    part = jnp.dot(high[...], rows, preferred_element_type=F32)
    part = part + jnp.dot(middle[...], rows, preferred_element_type=F32)
    part = part + jnp.dot(low[...], rows, preferred_element_type=F32)
    shared = shared_ref[...]
    half, feat = shared.shape[0], home_ref.shape[1]
    top = part[:half] + jnp.where(core == 0, shared, 0.0)
    bottom = part[half:] + jnp.where(core == 0, 0.0, shared)
    for at, value in ((slice(0, half), top), (slice(half, 2 * half), bottom)):
        left, right = value[:, :feat], value[:, feat:]
        home_ref[at, :] = jnp.where(core == 0, left, right)
        away_ref[at, :] = jnp.where(core == 0, right, left)


def arrive_kernel(rows_ref, own_ref, other_ref, gain_ref, first_ref, second_ref):
    core, _ = here()
    slots, width = rows_ref.shape
    half, feat = own_ref.shape[0] // 2, own_ref.shape[1]
    n_sub = (slots + half) // 2
    mine = pl.ds(pl.multiple_of(core * half, half), half)
    own, other = own_ref[mine, :], other_ref[mine, :]
    own, other = jnp.where(core == 0, own, other), jnp.where(core == 0, other, own)
    split = slots - n_sub
    gain = gain_ref[...]

    def put(ref, at, rows, columns):
        raw = rows.astype(F32)
        ref[at : at + rows.shape[0], columns] = (raw * gain[:, columns]).astype(BF)
        return raw * raw

    every, left, right = slice(0, width), slice(0, feat), slice(feat, width)

    def total(squares):
        ones = jnp.ones((SPARE, squares.shape[1]), BF)
        high, middle, low = (times(ones, part) for part in thirds(squares))
        return high + middle + low

    def spare(ref, at, sums):
        high, middle, low = thirds(sums)
        row = lax.broadcasted_iota(jnp.int32, sums.shape, 0)
        parts = jnp.where(row == 0, high.astype(F32), jnp.where(row == 1, middle.astype(F32), low.astype(F32)))
        ref[n_sub:, at : at + sums.shape[1]] = jnp.where(row < 3, parts, 0.0).astype(BF)

    for ref in (first_ref, second_ref):
        ref[n_sub:, :] = jnp.zeros((SPARE, width), BF)
    spare(first_ref, 0, total(put(first_ref, 0, rows_ref[:n_sub, :], every)))
    sums = total(put(second_ref, 0, rows_ref[n_sub:, :], every))
    tail = total(put(second_ref, split, own, left)) + total(put(second_ref, split, other, right))
    spare(second_ref, 0, jnp.concatenate([sums, tail], axis=1))


def early_kernel(places, spans, n_y, width, gate, up, s_gate, s_up, got, *refs):
    n = len(places)
    pieces = refs[:n]
    total_ref, squares_ref, w_last, sw_last, w, sw = refs[n:]
    core, y = here()
    hid = s_gate.shape[0]
    n_sub = total_ref.shape[0] // 2
    own = pl.multiple_of(core * hid, hid)
    other = pl.multiple_of((1 - core) * hid, hid)
    for i, (mine, into, base) in enumerate(
        ((gate.at[core], w, 0), (up.at[core], w, 2 * hid), (s_gate, sw, 0), (s_up, sw, 2 * hid))
    ):
        into[pl.ds(base + own, hid), :] = mine[...]
        into[pl.ds(base + other, hid), :] = got[i * hid : (i + 1) * hid, :]

    def columns(offset):
        return pl.ds(pl.multiple_of(lax.rem(y + offset + n_y, n_y) * width, width), width)

    for half in range(2):
        total = [None] * len(spans[half])
        squares = jnp.zeros((SPARE, width), F32)
        for piece, (k, offset) in zip(pieces, places):
            if k != half:
                continue
            for j, (low, high, which) in enumerate(spans[half]):
                term = times(piece[low:high, :], (w, sw)[which][:, columns(offset)])
                total[j] = term if total[j] is None else total[j] + term
            squares = squares + piece[n_sub:, :].astype(F32)
        for (low, high, _), value in zip(spans[half], total):
            total_ref[half * n_sub + low : half * n_sub + high, :] = value
        squares_ref[half * SPARE : (half + 1) * SPARE, :] = squares
    w_last[...] = w[:, columns(n_y // 2)]
    sw_last[...] = sw[:, columns(n_y // 2)]


def late_kernel(spans, features, w_ref, sw_ref, total_ref, squares_ref, *refs):
    out_ref = refs[-1]
    n_sub = total_ref.shape[0] // 2
    for half in range(2):
        piece = refs[half]
        squares = squares_ref[half * SPARE : (half + 1) * SPARE, :] + piece[n_sub:, :].astype(F32)
        squares = jnp.sum(squares, axis=0, keepdims=True)
        scale = lax.rsqrt(squares / features + EPSILON)
        scale = jnp.broadcast_to(scale, (128, scale.shape[1])).T
        for low, high, which in spans[half]:
            rows = slice(half * n_sub + low, half * n_sub + high)
            total = total_ref[rows, :] + times(piece[low:high, :], (w_ref, sw_ref)[which][...])
            n = total.shape[1] // 2
            gate, up = total[:, :n] * scale[low:high, :n], total[:, n:] * scale[low:high, :n]
            hidden = (gate / (1.0 + jnp.exp(-gate)) * up).astype(BF)
            for j in range(out_ref.shape[0]):
                out_ref[j, rows, :] = hidden


def down_kernel(hidden_ref, own_ref, got_ref, out_ref):
    core, _ = here()
    feat = own_ref.shape[2]
    slots = out_ref.shape[0]
    hidden = jnp.concatenate([hidden_ref[j, :slots, :] for j in range(hidden_ref.shape[0])], axis=1)
    for w, where in ((own_ref.at[core], core), (got_ref, 1 - core)):
        at = pl.ds(pl.multiple_of(where * feat, feat), feat)
        out_ref[:, at] = jnp.dot(
            hidden, w[: hidden.shape[1], :], preferred_element_type=F32
        ).astype(BF)


def pack_kernel(*refs):
    arrays, out_ref = refs[:-1], refs[-1]
    rows = out_ref.shape[0] // len(arrays)
    for i, a in enumerate(arrays):
        part = a.at[1 - here()[0]] if len(a.shape) == 3 else a
        out_ref[i * rows : (i + 1) * rows, :] = part[...]


def call(kernel, out, args, flops, mib, scratch=()):
    return pl.pallas_call(
        kernel,
        out_shape=out,
        in_specs=[VMEM] * len(args),
        out_specs=jax.tree.map(lambda _: VMEM, out),
        scratch_shapes=scratch,
        cost_estimate=pl.CostEstimate(flops=flops, bytes_accessed=2**21, transcendentals=0),
        compiler_params=pltpu.CompilerParams(vmem_limit_bytes=mib * 2**20),
    )(*args)


def body(
    tokens,
    pre_gain,
    expert_ids,
    route_weight,
    expert_gate,
    expert_up,
    expert_down,
    shared_gate,
    shared_up,
    shared_down,
    out_gain,
):
    tok, top = expert_ids.shape
    n_ep = lax.axis_size("ep")
    n_tp = lax.axis_size("tp")
    n_y = n_tp // 2
    experts = expert_gate.shape[0] * n_ep
    cap = 4 * tok * top // (3 * experts)
    feat = tokens.shape[1]
    feat_all = feat * n_tp
    width = 2 * feat
    hid = expert_gate.shape[1]
    n_hid = expert_down.shape[1]
    half = tok // 2
    slots = n_ep * cap
    rows = slots + half
    n_sub = rows // 2
    tp = lax.axis_index("tp")
    core = lax.rem(tp, 2)
    y = lax.div(tp, 2)
    first = core == 0

    swap = [(i, i ^ 1) for i in range(n_tp)]
    y_groups = [[c + 2 * k for k in range(n_y)] for c in range(2)]

    def y_shift(d):
        return [(i, ((i // 2 + d) % n_y) * 2 + i % 2) for i in range(n_tp)]

    def own_first(mine, other, axis):
        return jnp.where(
            first,
            jnp.concatenate([mine, other], axis=axis),
            jnp.concatenate([other, mine], axis=axis),
        )

    partner = lax.ppermute(tokens, "tp", swap)
    ids = expert_ids.T
    one_hot, own_part = call(
        functools.partial(own_kernel, n_ep, cap),
        (jax.ShapeDtypeStruct((slots, tok), BF), jax.ShapeDtypeStruct((slots, feat), BF)),
        (ids, tokens),
        10**8,
        8,
    )
    outgoing = call(
        join_kernel,
        jax.ShapeDtypeStruct((slots, width), BF),
        (one_hot, own_part, partner),
        10**8,
        8,
    )
    arrived = lax.all_to_all(outgoing.reshape(n_ep, cap, width), "ep", 0, 0, tiled=True)
    arrived = arrived.reshape(slots, width)

    gain = own_first(pre_gain, lax.ppermute(pre_gain, "tp", swap), 0)[None, :]
    sent_in = call(
        pack_kernel,
        jax.ShapeDtypeStruct((4 * hid, feat_all), BF),
        (expert_gate, expert_up, shared_gate, shared_up),
        4 * 10**8,
        8,
    )
    got_in = lax.ppermute(sent_in, "tp", swap)
    sent_out = call(
        pack_kernel,
        jax.ShapeDtypeStruct((2 * n_hid, feat), BF),
        (expert_down, shared_down),
        4 * 10**8,
        6,
    )
    got_out = lax.ppermute(sent_out, "tp", swap)

    piece = jax.ShapeDtypeStruct((n_sub + SPARE, width), BF)
    fwd = call(
        arrive_kernel, (piece, piece), (arrived, tokens, partner, gain), 4 * 10**8, 8
    )
    fwd, bwd = list(fwd), list(fwd)
    spans = (((0, n_sub, 0),), ((0, slots - n_sub, 0), (slots - n_sub, n_sub, 1)))
    early, early_at = list(fwd), [(0, 0), (1, 0)]
    late, late_at = [], []
    for step in range(1, n_y // 2 + 1):
        last = step == n_y // 2
        pieces, at = (late, late_at) if last else (early, early_at)
        for k in range(2):
            if not last or k == 0:
                fwd[k] = lax.ppermute(fwd[k], "tp", y_shift(1))
                pieces.append(fwd[k])
                at.append((k, -step))
            if not last or k == 1:
                bwd[k] = lax.ppermute(bwd[k], "tp", y_shift(-1))
                pieces.append(bwd[k])
                at.append((k, step))

    flops = 2 * rows * feat_all * 4 * hid
    total, squares, w_last, sw_last = call(
        functools.partial(early_kernel, early_at, spans, n_y, width),
        (
            jax.ShapeDtypeStruct((rows, 4 * hid), F32),
            jax.ShapeDtypeStruct((2 * SPARE, width), F32),
            jax.ShapeDtypeStruct((4 * hid, width), BF),
            jax.ShapeDtypeStruct((4 * hid, width), BF),
        ),
        (expert_gate, expert_up, shared_gate, shared_up, got_in, *early),
        flops,
        20,
        [pltpu.VMEM((4 * hid, feat_all), BF), pltpu.VMEM((4 * hid, feat_all), BF)],
    )
    hidden = call(
        functools.partial(late_kernel, spans, feat_all),
        jax.ShapeDtypeStruct((n_y, rows, 2 * hid), BF),
        (w_last, sw_last, total, squares, *late),
        flops // 8,
        8,
    )

    hidden_all = lax.all_to_all(hidden, "tp", 0, 0, axis_index_groups=y_groups, tiled=True)
    expert_out = call(
        down_kernel,
        jax.ShapeDtypeStruct((slots, width), BF),
        (hidden_all, expert_down, got_out),
        2 * slots * n_hid * width,
        12,
    )
    returned = lax.all_to_all(expert_out.reshape(n_ep, cap, width), "ep", 0, 0, tiled=True)
    returned = returned.reshape(slots, width)

    sdown_w = own_first(shared_down, got_out[n_hid:], 1).reshape(n_y, 2 * hid, width)
    contract = (((0, 2), (0, 1)), ((), ()))
    shared_out = lax.dot_general(hidden_all[:, slots:], sdown_w, contract, preferred_element_type=F32)
    third = jax.ShapeDtypeStruct((tok, slots), BF)
    mix = call(
        functools.partial(mix_kernel, n_ep, cap),
        (third, third, third),
        (ids, route_weight.T),
        4 * 10**8,
        60,
    )
    value = jax.ShapeDtypeStruct((tok, feat), F32)
    home, away = call(
        combine_kernel, (value, value), (*mix, returned, shared_out), 6 * tok * slots * width, 8
    )
    summed = home + lax.ppermute(away, "tp", swap)
    own_square = jnp.sum(summed * summed, axis=1)
    sent = jnp.broadcast_to(own_square[None, :], (n_tp, tok))
    out_square = jnp.sum(lax.all_to_all(sent, "tp", 0, 0, tiled=True), axis=0)
    return (summed * lax.rsqrt(out_square[:, None] / feat_all + EPSILON) * out_gain).astype(BF)


def solution(mesh):
    return jax.shard_map(
        body,
        mesh=mesh,
        in_specs=(
            P("ep", "tp"),
            P("tp"),
            P("ep", None),
            P("ep", None),
            P("ep", "tp", None),
            P("ep", "tp", None),
            P("ep", None, "tp"),
            P("tp", None),
            P("tp", None),
            P(None, "tp"),
            P("tp"),
        ),
        out_specs=P("ep", "tp"),
        check_vma=False,
    )
```
